32 devices in a mesh: ep: 8 (over z, x), tp: 4 (over y, core).
Axes of the slice: x: 2, y: 2, z: 4, core: 2. Of those that a mesh axis runs over, the one named last changes fastest.
Arguments:
- tokens: bfloat16 [128, 2048], P('ep'), may hold values from -120 to 120
- lengths: int32 [128], P('ep'), may hold values from 1 to 768, as said below
- cache_kv: bfloat16 [128, 768, 16, 128], P('ep', None, 'tp'), may hold values from -64 to 64
- cache_cum: float32 [128, 16, 768], P('ep', 'tp'), may hold values from -768 to 0, as said below
- norm_attn: float32 [2048], replicated, may hold values from 0.1 to 1.9
- w_query: bfloat16 [2048, 1024], P(None, 'tp'), may hold values from -0.125 to 0.125
- w_key: bfloat16 [2048, 1024], P(None, 'tp'), may hold values from -0.125 to 0.125
- w_value: bfloat16 [2048, 1024], P(None, 'tp'), may hold values from -0.125 to 0.125
- w_forget: bfloat16 [2048, 16], P(None, 'tp'), may hold values from -0.125 to 0.125
- b_forget: float32 [16], P('tp'), may hold values from -1 to 2
- w_output: bfloat16 [1024, 2048], P('tp'), may hold values from -0.1875 to 0.1875
- norm_ffn: float32 [2048], replicated, may hold values from 0.1 to 1.9
- shared_gate: bfloat16 [2048, 512], P(None, 'tp'), may hold values from -0.125 to 0.125
- shared_up: bfloat16 [2048, 512], P(None, 'tp'), may hold values from -0.125 to 0.125
- shared_down: bfloat16 [512, 2048], P('tp'), may hold values from -0.25 to 0.25
- expert_gate: bfloat16 [24, 2048, 512], P('ep', None, 'tp'), may hold values from -0.125 to 0.125
- expert_up: bfloat16 [24, 2048, 512], P('ep', None, 'tp'), may hold values from -0.125 to 0.125
- expert_down: bfloat16 [24, 512, 2048], P('ep', 'tp'), may hold values from -0.25 to 0.25
- route_ids: int32 [128, 6], P('ep'), may hold values from 0 to 23, all different within a row; in each aligned block of 16 rows (0 to 15, 16 to 31, ...) at most 8 rows name the same one
- route_weight: float32 [128, 6], P('ep'), may hold values from 0.1 to 0.8
Outputs:
- output: bfloat16 [128, 2048], P('ep', 'tp')
- new_kv: bfloat16 [128, 16, 128], P('ep', 'tp')
- new_cum: float32 [128, 16], P('ep', 'tp')
The draws below stay inside these ranges and needn't reach their ends.
Inputs may be any that keep to these rules, and one draw needn't show every extreme that they name: `lengths`: every block of 16 sequences of one index of ep holds one with 768. `route_ids`: in the rows of one device (aligned blocks of 16 rows) no expert is named more than 8 times. `cache_cum`: Non-increasing along positions.
All inputs are finite; a program needn't handle non-finite values.
Results may differ from the reference program's by a relative error of at most 0.012.
Values may be sent and summed in bfloat16 or wider, within the bound.
No kernel may reach another device: no remote copies, remote signals or barrier semaphores. Data moves between devices by JAX's collectives and lax.ppermute only.
A program may use at most 128 MiB of HBM per device.

```python
import math
import jax
import jax.numpy as jnp
import numpy as np
from jax import lax

D = 2048
ATTENTION_HEADS = 16
HEAD_DIM = 64
EF = 512
SF = 512
TOPK = 6
SEQ_DEV = 16
CACHE_POSITIONS = 768
SEQUENCE_COUNT = 128
EXPERTS = 24
CAP = 8
N_EP = 8
N_TP = 4


def length_draw(key):
    base_key = jax.random.fold_in(key, 11)
    drawn = jax.random.randint(base_key, (SEQUENCE_COUNT,), 1, CACHE_POSITIONS + 1)
    filled = jnp.arange(SEQUENCE_COUNT, dtype=jnp.int32) % SEQ_DEV == 0
    return jnp.where(filled, CACHE_POSITIONS, drawn).astype(jnp.int32)


def draw_lengths(key, part):
    return length_draw(key)


def draw_tokens(key, part):
    column_key = jax.random.fold_in(key, 41)
    row_key = jax.random.fold_in(key, 42)
    noise_key = jax.random.fold_in(key, 43)
    columns = jnp.arange(D, dtype=jnp.float32)
    column_scale = 0.3 * jnp.exp(jnp.log(10.0) * columns / D) * jnp.exp(jax.random.uniform(column_key, (D,), jnp.float32, -0.7, 0.7))
    row_scale = jnp.exp(jax.random.uniform(row_key, (SEQUENCE_COUNT, 1), jnp.float32, jnp.log(0.3), jnp.log(3.0)))
    noise_draw = jnp.clip(jax.random.normal(noise_key, (SEQUENCE_COUNT, D), jnp.float32), -6.0, 6.0)
    return (noise_draw * row_scale * column_scale[None, :]).astype(jnp.bfloat16)


def draw_cache_kv(key, part):
    noise_key = jax.random.fold_in(key, 21)
    shape = (SEQUENCE_COUNT, CACHE_POSITIONS, ATTENTION_HEADS, 2 * HEAD_DIM)
    values = jnp.clip(jax.random.normal(noise_key, shape, jnp.float32), -6.0, 6.0)
    return values.astype(jnp.bfloat16)


def draw_cache_cum(key, part):
    head_key = jax.random.fold_in(key, 31)
    factor_key = jax.random.fold_in(key, 32)
    rough_key = jax.random.fold_in(key, 33)
    spike_random_key = jax.random.fold_in(key, 34)
    height_random_key = jax.random.fold_in(key, 35)
    slow_share = 0.5
    slow = jax.random.uniform(head_key, (SEQUENCE_COUNT, ATTENTION_HEADS)) < slow_share
    seq_factor = jnp.exp(jax.random.uniform(factor_key, (SEQUENCE_COUNT, 1), jnp.float32, -0.7, 0.7))
    falloff_speed = jnp.where(slow, 0.5 / CACHE_POSITIONS, 1.0 / 40.0) * seq_factor
    jaggedness = jnp.exp(jax.random.uniform(rough_key, (SEQUENCE_COUNT, ATTENTION_HEADS, CACHE_POSITIONS), jnp.float32, -1.1, 1.1))
    spike_mask = jax.random.uniform(spike_random_key, (SEQUENCE_COUNT, ATTENTION_HEADS, CACHE_POSITIONS)) < 2.0 / CACHE_POSITIONS
    spike_height = jax.random.uniform(height_random_key, (SEQUENCE_COUNT, ATTENTION_HEADS, CACHE_POSITIONS), jnp.float32, 0.22, 0.69)
    stride_amounts = falloff_speed[:, :, None] * jaggedness + jnp.where(spike_mask, spike_height, 0.0)
    return -jnp.cumsum(stride_amounts, axis=2)


def level_of(rng, shape, cuts, low, top_value):
    loudness, own = 1.0, jax.random.fold_in(rng, 6)
    for position, parts in cuts:
        draws = jnp.exp(jax.random.uniform(jax.random.fold_in(own, position), (parts,), jnp.float32, low / len(cuts), top_value / len(cuts)))
        loudness = loudness * jnp.repeat(draws, shape[position] // parts).reshape([-1 if axis == position else 1 for axis in range(len(shape))])
    return loudness


def assign_block(key, own, number, rows, count, top, reach, lean):
    ranking = jax.random.permutation(key, count)
    heavy_load, common = shares(count, rows * top, reach, lean, True), shares(count, rows * top, reach, lean, False)
    places = jnp.arange(count)

    def named(tallies, offset_by):
        used = int((tallies > 0).sum())
        fixed = max(1, used // 4)
        shifted = fixed + (places - fixed + offset_by * (used - fixed)) % max(1, count - fixed)
        return jnp.zeros((count,), jnp.int32).at[ranking[jnp.where(places < fixed, places, shifted)]].set(jnp.asarray(tallies, jnp.int32))

    tallies = jnp.where(number % 4 == 0, named(heavy_load, number // 4), named(common, number - number // 4 - 1))
    mixed = jax.random.permutation(jax.random.fold_in(own, 3), count)
    source_of, taker = mixed[0:count // 2 * 2:2], mixed[1:count // 2 * 2:2]
    margin = jnp.minimum(tallies[source_of] - 1, reach - tallies[taker]) // 2
    margin = jnp.where((source_of == ranking[0]) | (taker == ranking[0]) | (tallies[taker] == 0), 0, jnp.maximum(margin, 0))
    shifted = jax.random.randint(jax.random.fold_in(own, 4), (count // 2,), 0, 1 << 20) % (margin + 1)
    tallies = tallies.at[source_of].add(-shifted).at[taker].add(shifted)
    items = jnp.searchsorted(jnp.cumsum(tallies), jnp.arange(rows * top), side="right").astype(jnp.int32)
    listing = items.reshape(top, rows).T
    listing = listing[jax.random.permutation(jax.random.fold_in(own, 1), rows)]
    offset_by = jax.random.randint(jax.random.fold_in(own, 2), (rows, 1), 0, top)
    return jnp.take_along_axis(listing, (jnp.arange(top)[None, :] + offset_by) % top, axis=1)


def shares(amount, total, limit, slope, full):
    weights = [(1 << 20) // math.isqrt(standing ** slope) + 1 for standing in range(1, amount + 1)]
    largest = limit if full else min(limit, max(-(-total // amount), total * weights[0] // sum(weights)))
    least = 1 if total - largest >= amount - 1 else 0
    given, spare = [largest] + [least] * (amount - 1), total - largest - least * (amount - 1)
    while spare > 0:
        candidates = [i for i in range(1, amount) if given[i] < largest] or [i for i in range(1, amount) if given[i] < limit]
        pool, remaining = sum([weights[i] for i in candidates]), spare
        for i in candidates:
            more = min(limit - given[i], max(1, remaining * weights[i] // pool), spare)
            given[i] = given[i] + more
            spare = spare - more
    return np.array(given)


def normal_values(rng, dims, width, limit, shards=(), kind=jnp.bfloat16):
    values = jax.random.normal(rng, dims, jnp.float32) * width
    if len(shards) > 0:
        values = level_of(rng, dims, shards, -0.22, 0.18) * values
    return jnp.clip(values, min=-limit, max=limit).astype(kind)


def setup_inputs(seed: int = 0) -> dict:
    key_of = jax.random.split(jax.random.key(seed), 21)
    tokens = draw_tokens(jax.random.fold_in(key_of[20], 71), 0)
    lengths = draw_lengths(jax.random.fold_in(key_of[20], 71), 0)
    cache_kv = draw_cache_kv(jax.random.fold_in(key_of[20], 71), 0)
    cache_cum = draw_cache_cum(jax.random.fold_in(key_of[20], 71), 0)
    norm_attn = jnp.clip(1.0 + 0.18 * jax.random.normal(key_of[4], (D,), jnp.float32), 0.1, 1.9)
    w_query = normal_values(key_of[5], (D, ATTENTION_HEADS * HEAD_DIM), D ** -0.5, 0.125, ((1, 4),))
    w_key = normal_values(key_of[6], (D, ATTENTION_HEADS * HEAD_DIM), D ** -0.5, 0.125, ((1, 4),))
    w_value = normal_values(key_of[7], (D, ATTENTION_HEADS * HEAD_DIM), D ** -0.5, 0.125, ((1, 4),))
    w_forget = normal_values(key_of[8], (D, ATTENTION_HEADS), D ** -0.5, 0.125, ((1, 4),))
    b_forget = jnp.clip(-1.0 + 3.0 * jax.random.uniform(key_of[9], (ATTENTION_HEADS,), jnp.float32) ** level_of(key_of[9], (ATTENTION_HEADS,), ((0, 4),), -0.2, 0.2), -1.0, 2.0)
    w_output = normal_values(key_of[10], (ATTENTION_HEADS * HEAD_DIM, D), (ATTENTION_HEADS * HEAD_DIM) ** -0.5, 0.1875, ((0, 4),))
    norm_ffn = jnp.clip(1.0 + 0.18 * jax.random.normal(key_of[11], (D,), jnp.float32), 0.1, 1.9)
    shared_gate = normal_values(key_of[12], (D, SF), D ** -0.5, 0.125, ((1, 4),))
    shared_up = normal_values(key_of[13], (D, SF), D ** -0.5, 0.125, ((1, 4),))
    shared_down = normal_values(key_of[14], (SF, D), SF ** -0.5, 0.25, ((0, 4),))
    expert_gate = normal_values(key_of[15], (EXPERTS, D, EF), D ** -0.5, 0.125, ((0, 8), (2, 4)))
    expert_up = normal_values(key_of[16], (EXPERTS, D, EF), D ** -0.5, 0.125, ((0, 8), (2, 4)))
    expert_down = normal_values(key_of[17], (EXPERTS, EF, D), EF ** -0.5, 0.25, ((0, 8), (1, 4)))
    route_ids_keys = jax.random.split(jax.random.fold_in(key_of[18], 1), SEQUENCE_COUNT // SEQ_DEV)
    route_ids_turns = jax.random.permutation(jax.random.fold_in(key_of[18], 3), SEQUENCE_COUNT // SEQ_DEV)
    route_ids = jax.vmap(lambda own, number: assign_block(jax.random.fold_in(key_of[18], 2), own, number, SEQ_DEV, EXPERTS, TOPK, CAP, 1))(route_ids_keys, route_ids_turns).reshape((SEQUENCE_COUNT, TOPK))
    route_weight = jnp.clip(jnp.exp(math.log(0.8) - 2.0794415 * jax.random.uniform(key_of[19], (SEQUENCE_COUNT, TOPK), jnp.float32) ** level_of(key_of[19], (SEQUENCE_COUNT, TOPK), ((0, 8),), -0.2, 0.2)), 0.1, 0.8)
    return {"tokens": tokens, "lengths": lengths, "cache_kv": cache_kv, "cache_cum": cache_cum, "norm_attn": norm_attn, "w_query": w_query, "w_key": w_key, "w_value": w_value, "w_forget": w_forget, "b_forget": b_forget, "w_output": w_output, "norm_ffn": norm_ffn, "shared_gate": shared_gate, "shared_up": shared_up, "shared_down": shared_down, "expert_gate": expert_gate, "expert_up": expert_up, "expert_down": expert_down, "route_ids": route_ids, "route_weight": route_weight}


epsilon = 1e-06

def rms_scale(row_block, gain):
    widened = row_block.astype(jnp.float32)
    return widened * lax.rsqrt(lax.optimization_barrier(jnp.mean(widened * widened, axis=-1, keepdims=True)) + epsilon) * gain

def split_sum(hidden, weight):
    row_count = hidden.shape[0]
    pieces = jnp.einsum('rtf,tfd->rtd', hidden.reshape(row_count, N_TP, -1).astype(jnp.float32), weight.reshape(N_TP, -1, weight.shape[1]).astype(jnp.float32))
    rounded = lax.optimization_barrier(pieces.astype(jnp.bfloat16))
    return lax.optimization_barrier(jnp.sum(rounded.astype(jnp.float32), axis=1))

def expert_apply(row_block, w_gate, w_up, w_down):
    gate_value = jnp.dot(row_block, w_gate, preferred_element_type=jnp.float32)
    up_value = jnp.dot(row_block, w_up, preferred_element_type=jnp.float32)
    hidden = (jax.nn.silu(gate_value) * up_value).astype(jnp.bfloat16)
    return split_sum(hidden, w_down)

def attend_one(inputs):
    queries, key_new, value_new, cache_rows, cum_rows, length, cum_new = inputs
    score_scale = HEAD_DIM ** (-0.5)
    keys_past = cache_rows[:, :, :HEAD_DIM].astype(jnp.float32)
    values_past = cache_rows[:, :, HEAD_DIM:].astype(jnp.float32)
    widened = queries.astype(jnp.float32)
    past_scores = jnp.einsum('hd,lhd->hl', widened, keys_past) * score_scale
    past_scores = past_scores + cum_new[:, None] - cum_rows
    is_valid = jnp.arange(CACHE_POSITIONS, dtype=jnp.int32)[None, :] < length
    past_scores = jnp.where(is_valid, past_scores, -jnp.inf)
    own_score = lax.optimization_barrier(jnp.sum(widened * key_new.astype(jnp.float32), axis=1)) * score_scale
    row_max = jnp.maximum(lax.optimization_barrier(jnp.max(past_scores, axis=1)), own_score)
    weights_past = jnp.exp(past_scores - row_max[:, None])
    weight_own = jnp.exp(own_score - row_max)
    weight_sum = lax.optimization_barrier(jnp.sum(weights_past, axis=1)) + weight_own
    probs_past = (weights_past / weight_sum[:, None]).astype(jnp.bfloat16)
    prob_own = (weight_own / weight_sum).astype(jnp.bfloat16)
    mixed = jnp.einsum('hl,lhd->hd', probs_past.astype(jnp.float32), values_past)
    mixed = mixed + prob_own.astype(jnp.float32)[:, None] * value_new.astype(jnp.float32)
    return mixed.astype(jnp.bfloat16)

def run_expert(inputs):
    return expert_apply(*inputs).astype(jnp.bfloat16)

def reference(tokens, lengths, cache_kv, cache_cum, norm_attn, w_query, w_key, w_value, w_forget, b_forget, w_output, norm_ffn, shared_gate, shared_up, shared_down, expert_gate, expert_up, expert_down, route_ids, route_weight):
    seq_total = tokens.shape[0]
    normed = rms_scale(tokens, norm_attn).astype(jnp.bfloat16)
    queries = jnp.dot(normed, w_query, preferred_element_type=jnp.float32).astype(jnp.bfloat16).reshape(seq_total, ATTENTION_HEADS, HEAD_DIM)
    key_new = jnp.dot(normed, w_key, preferred_element_type=jnp.float32).astype(jnp.bfloat16).reshape(seq_total, ATTENTION_HEADS, HEAD_DIM)
    value_new = jnp.dot(normed, w_value, preferred_element_type=jnp.float32).astype(jnp.bfloat16).reshape(seq_total, ATTENTION_HEADS, HEAD_DIM)
    forget_log = jax.nn.log_sigmoid(jnp.dot(normed, w_forget, preferred_element_type=jnp.float32) + b_forget)
    last_index = jnp.broadcast_to((lengths - 1)[:, None, None], (seq_total, ATTENTION_HEADS, 1)).astype(jnp.int32)
    cum_new = jnp.take_along_axis(cache_cum, last_index, axis=2)[:, :, 0] + forget_log
    attended = lax.map(attend_one, (queries, key_new, value_new, cache_kv, cache_cum, lengths, cum_new))
    attended = attended.reshape(seq_total, ATTENTION_HEADS * HEAD_DIM)
    residual = (tokens.astype(jnp.float32) + split_sum(attended, w_output)).astype(jnp.bfloat16)
    ffn_in = rms_scale(residual, norm_ffn).astype(jnp.bfloat16)
    shared_out = expert_apply(ffn_in, shared_gate, shared_up, shared_down)
    route_flat = route_ids.reshape(N_EP, SEQ_DEV * TOPK)
    onehot = (route_flat[:, :, None] == jnp.arange(EXPERTS, dtype=jnp.int32)[None, None, :]).astype(jnp.int32)
    before = jnp.cumsum(onehot, axis=1) - onehot
    slot_rank = lax.optimization_barrier(jnp.sum(before * onehot, axis=2))
    group_index = jnp.arange(N_EP, dtype=jnp.int32)[:, None]
    slot_index = ((route_flat * N_EP + group_index) * CAP + slot_rank).reshape(-1).astype(jnp.int32)
    token_of_route = jnp.repeat(jnp.arange(seq_total, dtype=jnp.int32), TOPK)
    buffer = jnp.zeros((EXPERTS * N_EP * CAP, D), jnp.bfloat16).at[slot_index].set(ffn_in[token_of_route])
    expert_rows = buffer.reshape(EXPERTS, N_EP * CAP, D)
    expert_out = lax.map(run_expert, (expert_rows, expert_gate, expert_up, expert_down))
    picked = expert_out.reshape(-1, D)[slot_index].reshape(seq_total, TOPK, D).astype(jnp.float32)
    routed = lax.optimization_barrier(jnp.sum(picked * route_weight[:, :, None], axis=1))
    output = (residual.astype(jnp.float32) + shared_out + routed).astype(jnp.bfloat16)
    new_kv = jnp.concatenate([key_new, value_new], axis=2)
    return (output, new_kv, cum_new)
```

```python
import jax
import jax.numpy as jnp
from jax import lax
from jax.experimental import pallas as pl
from jax.experimental.pallas import tpu as pltpu
from jax.sharding import Mesh, PartitionSpec as P

HEAD_DIM = 64
CORES = 2
LANES = 128
EPSILON = 1e-06
HUGE = 1 << 30
BATCH = 4
TENSOR = ("ty", "tc")

f32 = jnp.float32
bf16 = jnp.bfloat16

NT = (((1,), (1,)), ((), ()))


def field(count):
    return -(-count // 8) * 8


def full_spec():
    return pl.BlockSpec(memory_space=pltpu.VMEM)


def hbm_spec():
    return pl.BlockSpec(memory_space=pltpu.HBM)


def smem_spec():
    return pl.BlockSpec(memory_space=pltpu.SMEM)


def attention_kernel(
    tokens_in,
    norm_in,
    w_forget_in,
    cum_in,
    lengths_in,
    b_forget_in,
    ids_in,
    route_in,
    w_query,
    w_key,
    w_value,
    w_output,
    cache,
    *refs,
    carried,
):
    carry_in, refs = refs[:carried], refs[carried:]
    mine_out, other_out, kv_out, cum_out, meta_out = refs[:5]
    carry_out, refs = refs[5 : 5 + carried], refs[5 + carried :]
    (
        tokens,
        norm_attn,
        w_forget,
        cum,
        lengths,
        b_forget,
        ids,
        route,
        wq_buf,
        wk_buf,
        wv_buf,
        wo_buf,
        cache_buf,
        q_rows,
        kv_rows,
        att_rows,
        bias_buf,
        shift_buf,
        score_buf,
        meta_rows,
        sem_w,
        sem_c,
        sem_n,
    ) = refs
    seq, width = tokens.shape
    heads, length = cum.shape[1:]
    half_rows = cache.shape[1] // 2
    half_len = length // 2
    tiles = half_len // LANES
    span = LANES * heads
    pair = 2 * heads
    parts, _, part = mine_out.shape

    moves = (
        (tokens_in, tokens),
        (norm_in, norm_attn),
        (w_forget_in, w_forget),
        (lengths_in, lengths),
        (b_forget_in, b_forget),
        (ids_in, ids),
        (route_in, route),
        (cum_in, cum),
        (w_query, wq_buf),
        (w_key, wk_buf),
        (w_value, wv_buf),
        (w_output, wo_buf),
    )
    w_copies = [
        pltpu.make_async_copy(src, dst, sem_w.at[i]) for i, (src, dst) in enumerate(moves)
    ]
    c_copies = [
        pltpu.make_async_copy(cache.at[s], cache_buf.at[s], sem_c.at[s]) for s in range(seq)
    ]
    n_copies = [
        pltpu.make_async_copy(src, dst, sem_n.at[i])
        for i, (src, dst) in enumerate(zip(carry_in, carry_out))
    ]
    for copy in w_copies[:-1]:
        copy.start()
    for copy in c_copies:
        copy.start()
    w_copies[-1].start()
    for copy in n_copies:
        copy.start()

    sub = lax.broadcasted_iota(jnp.int32, (LANES, span), 0) * heads
    lane = lax.broadcasted_iota(jnp.int32, (LANES, span), 1)
    spread = ((lane >= sub) & (lane < sub + heads)).astype(f32).astype(bf16)
    row_id = lax.broadcasted_iota(jnp.int32, (pair, half_rows), 0)
    col_id = lax.broadcasted_iota(jnp.int32, (pair, half_rows), 1)
    place = jnp.where(
        lax.rem(row_id, heads) == lax.rem(col_id, heads),
        col_id + jnp.where(row_id >= heads, half_rows, 0),
        HUGE,
    )
    seq_lane = lax.broadcasted_iota(jnp.int32, (heads, seq), 1)
    pos_lane = lax.broadcasted_iota(jnp.int32, (heads, length), 1)
    head_row = lax.broadcasted_iota(jnp.int32, (heads, 1), 0)

    for copy in w_copies[:7]:
        copy.wait()
    wide = tokens[...].astype(f32)
    scale = lax.rsqrt(jnp.mean(wide * wide, axis=1, keepdims=True) + EPSILON)
    normed = (wide * scale * norm_attn[...]).astype(bf16)
    gate = lax.dot_general(w_forget[...], normed, NT, preferred_element_type=f32)
    for h in range(heads):
        gate = gate + jnp.where(head_row == h, b_forget[h], 0.0)
    forget_log = jnp.minimum(gate, 0.0) - jnp.log1p(jnp.exp(-jnp.abs(gate)))

    top_count = ids.shape[0]
    stride = field(top_count)
    meta_rows[...] = jnp.zeros_like(meta_rows)
    high = route[...].astype(bf16).astype(f32)
    middle = (route[...] - high).astype(bf16).astype(f32)
    for i, value in enumerate((ids[...].astype(f32), high, middle, route[...] - high - middle)):
        meta_rows[i * stride : i * stride + top_count, :] = value
    same = lax.broadcasted_iota(jnp.int32, (seq, seq), 0) == lax.broadcasted_iota(
        jnp.int32, (seq, seq), 1
    )
    meta_out[...] = lax.dot_general(
        same.astype(f32).astype(bf16),
        meta_rows[...].astype(bf16),
        NT,
        preferred_element_type=f32,
    ).astype(bf16)

    w_copies[7].wait()
    pieces = []
    for s in range(seq):
        rows = cum[s]
        for j in range(tiles):
            pieces.append(rows[:, j * LANES : (j + 1) * LANES])
            pieces.append(rows[:, half_len + j * LANES : half_len + (j + 1) * LANES])
    stacked = jnp.concatenate(pieces, axis=0)
    hi = stacked.astype(bf16)
    rest = stacked - hi.astype(f32)
    mid = rest.astype(bf16)
    low = (rest - mid.astype(f32)).astype(bf16)
    bias_buf[...] = (
        jnp.dot(hi, spread, preferred_element_type=f32)
        + jnp.dot(mid, spread, preferred_element_type=f32)
        + jnp.dot(low, spread, preferred_element_type=f32)
    )
    cum_all = jnp.zeros((heads, seq), f32)
    for s in range(seq):
        limit = lengths[s]
        last = jnp.sum(jnp.where(pos_lane == limit - 1, cum[s], 0.0), axis=1, keepdims=True)
        cum_new = last + forget_log[:, s : s + 1]
        cum_all = jnp.where(seq_lane == s, cum_new, cum_all)
        cum_two = jnp.concatenate([cum_new, cum_new], axis=0)
        base = s * tiles * pair
        bias = jnp.concatenate(
            [bias_buf[base + j * pair : base + (j + 1) * pair, :] for j in range(tiles)], axis=1
        )
        shift_buf[s] = jnp.where(place < limit * heads, cum_two - bias, -jnp.inf)
    cum_out[...] = cum_all

    w_copies[8].wait()
    query = jnp.dot(normed, wq_buf[...], preferred_element_type=f32).astype(bf16).astype(f32)
    w_copies[9].wait()
    key = jnp.dot(normed, wk_buf[...], preferred_element_type=f32).astype(bf16).astype(f32)
    w_copies[10].wait()
    value = jnp.dot(normed, wv_buf[...], preferred_element_type=f32).astype(bf16).astype(f32)
    for h in range(heads):
        cut = slice(h * HEAD_DIM, (h + 1) * HEAD_DIM)
        where_h = pl.ds(h, seq, stride=heads)
        q_rows[where_h, :] = jnp.concatenate(
            [query[:, cut] * HEAD_DIM ** (-0.5), jnp.zeros((seq, HEAD_DIM), f32)], axis=1
        )
        kv_rows[where_h, :] = jnp.concatenate([key[:, cut], value[:, cut]], axis=1)
    kv_out[...] = kv_rows[...].astype(bf16)

    def rows_of(s):
        return jnp.concatenate([cache_buf[s, :half_rows, :], cache_buf[s, half_rows:, :]], axis=1)

    def score(s):
        q_s = q_rows[s * heads : (s + 1) * heads, :]
        blank = jnp.zeros_like(q_s)
        lhs = jnp.concatenate(
            [jnp.concatenate([q_s, blank], axis=1), jnp.concatenate([blank, q_s], axis=1)], axis=0
        ).astype(bf16)
        score_buf[s] = lax.dot_general(lhs, rows_of(s), NT, preferred_element_type=f32)

    def attend(s):
        here = slice(s * heads, (s + 1) * heads)
        kv_s = kv_rows[here, :]
        own = jnp.sum(q_rows[here, :] * kv_s, axis=1, keepdims=True)
        scores = score_buf[s] + shift_buf[s]
        top = jnp.max(scores, axis=1, keepdims=True)
        top = jnp.maximum(jnp.maximum(top[:heads], top[heads:]), own)
        weights = jnp.exp(scores - jnp.concatenate([top, top], axis=0))
        weight_own = jnp.exp(own - top)
        total = jnp.sum(weights, axis=1, keepdims=True)
        inverse = 1.0 / (total[:heads] + total[heads:] + weight_own)
        probs = (weights * jnp.concatenate([inverse, inverse], axis=0)).astype(bf16)
        prob_own = (weight_own * inverse).astype(bf16).astype(f32)
        mixed = jnp.dot(probs, rows_of(s), preferred_element_type=f32)
        att_rows[here, :] = mixed[:heads, :LANES] + mixed[heads:, LANES:] + prob_own * kv_s

    for start in range(0, seq + BATCH, BATCH):
        if start < seq:
            for s in range(start, start + BATCH):
                c_copies[s].wait()
            for s in range(start, start + BATCH):
                score(s)
        if start:
            for s in range(start - BATCH, start):
                attend(s)

    attended = jnp.concatenate(
        [att_rows[pl.ds(h, seq, stride=heads), :][:, HEAD_DIM:] for h in range(heads)], axis=1
    ).astype(bf16)
    w_copies[11].wait()
    core = lax.rem(lax.axis_index(TENSOR), CORES)
    for y in range(parts):
        here = pl.ds(pl.multiple_of((y * CORES + core) * part, part), part)
        mine_out[y] = jnp.dot(attended, wo_buf[:, here], preferred_element_type=f32).astype(bf16)
        there = pl.ds(pl.multiple_of((y * CORES + 1 - core) * part, part), part)
        other_out[y] = jnp.dot(attended, wo_buf[:, there], preferred_element_type=f32).astype(bf16)
    for copy in n_copies:
        copy.wait()


def residual_kernel(*refs, groups):
    mine = refs[0]
    arrived = refs[1 : 1 + groups - 1]
    tokens, meta, packed_out, residual_out = refs[groups:]
    parts, _, part = mine.shape
    place = lax.axis_index(TENSOR)
    core = lax.rem(place, CORES)
    for y in range(parts):
        here = pl.ds(pl.multiple_of((y * CORES + core) * part, part), part)
        total = mine[y].astype(f32)
        for ref in arrived:
            total = total + ref[y].astype(f32)
        rounded = (tokens[:, here].astype(f32) + total).astype(bf16)
        for e in range(packed_out.shape[0]):
            packed_out[e, :, y * part : (y + 1) * part] = rounded

        @pl.when(place == y * CORES + core)
        def _():
            residual_out[...] = rounded

    for e in range(packed_out.shape[0]):
        packed_out[e, :, parts * part :] = meta[...]


def expert_kernel(
    near,
    far,
    norm_ffn,
    shared_gate,
    shared_up,
    shared_down,
    expert_gate,
    expert_up,
    expert_down,
    keep_out,
    send_out,
    rows_buf,
    *,
    top_count,
    seq,
):
    groups, parts, _, part = keep_out.shape
    row_count = near.shape[0]
    width = rows_buf.shape[1]
    core = lax.rem(lax.axis_index(TENSOR), CORES)
    group = lax.axis_index("ep")
    experts = expert_gate.shape[0]
    hidden = expert_gate.shape[2]

    squares = jnp.zeros((row_count, 1), f32)
    for ref in (near, far):
        for y in range(parts):
            piece = ref[:, y * part : (y + 1) * part].astype(f32)
            squares = squares + jnp.sum(piece * piece, axis=1, keepdims=True)
    scale = lax.rsqrt(squares * (1.0 / width) + EPSILON)
    for ref, side in ((near, core), (far, 1 - core)):
        for y in range(parts):
            here = pl.ds(pl.multiple_of((y * CORES + side) * part, part), part)
            piece = ref[:, y * part : (y + 1) * part].astype(f32)
            rows_buf[:, here] = (piece * scale * norm_ffn[:, here]).astype(bf16)

    meta = near[:, parts * part :].astype(f32)
    ids = meta[:, :top_count]
    stride = field(top_count)
    coef = (
        meta[:, stride : stride + top_count]
        + meta[:, 2 * stride : 2 * stride + top_count]
        + meta[:, 3 * stride : 3 * stride + top_count]
    )
    row_id = lax.broadcasted_iota(jnp.int32, (row_count, 1), 0)
    own = (row_id >= group * seq) & (row_id < (group + 1) * seq)
    rows = rows_buf[...]
    lane_full = hidden % LANES == 0

    def hidden_units(w_gate, w_up, factor):
        if lane_full:
            both = jnp.dot(
                rows, jnp.concatenate([w_gate, w_up], axis=1), preferred_element_type=f32
            )
            gate, up = both[:, :hidden], both[:, hidden:]
        else:
            gate = jnp.dot(rows, w_gate, preferred_element_type=f32)
            up = jnp.dot(rows, w_up, preferred_element_type=f32)
        return (gate / (1.0 + jnp.exp(-gate)) * up * factor).astype(bf16)

    units = []
    for e in range(experts):
        wanted = (group * experts + e).astype(f32)
        factor = jnp.sum(jnp.where(ids == wanted, coef, 0.0), axis=1, keepdims=True)
        units.append(hidden_units(expert_gate[e], expert_up[e], factor))
    units.append(hidden_units(shared_gate[...], shared_up[...], own.astype(f32)))
    if lane_full:
        joined = jnp.concatenate(units, axis=1)

    def down(here):
        blocks = [expert_down[e, :, here] for e in range(experts)] + [shared_down[:, here]]
        if lane_full:
            return jnp.dot(joined, jnp.concatenate(blocks, axis=0), preferred_element_type=f32)
        total = jnp.dot(units[0], blocks[0], preferred_element_type=f32)
        for unit, block in zip(units[1:], blocks[1:]):
            total = total + jnp.dot(unit, block, preferred_element_type=f32)
        return total

    for out, side in ((send_out, 1 - core), (keep_out, core)):
        for y in range(parts):
            here = pl.ds(pl.multiple_of((y * CORES + side) * part, part), part)
            result = down(here)
            for g in range(groups):
                out[g, y] = result[g * seq : (g + 1) * seq].astype(out.dtype)


def solution(mesh):
    groups = mesh.shape["ep"]
    tensor = mesh.shape["tp"]
    parts = tensor // CORES
    fine = Mesh(mesh.devices.reshape(groups, parts, CORES), ("ep", "ty", "tc"))

    def shards(
        tokens,
        lengths,
        cache_kv,
        cache_cum,
        norm_attn,
        w_query,
        w_key,
        w_value,
        w_forget,
        b_forget,
        w_output,
        norm_ffn,
        shared_gate,
        shared_up,
        shared_down,
        expert_gate,
        expert_up,
        expert_down,
        route_ids,
        route_weight,
    ):
        seq, width = tokens.shape
        heads, length = cache_cum.shape[1:]
        part = width // tensor
        rows = length * heads
        column = heads * HEAD_DIM
        half_shape = jax.ShapeDtypeStruct((parts, seq, part), bf16)
        carry = (shared_gate, shared_up, shared_down, expert_gate, expert_up, expert_down)
        mine, other, kv_flat, cum_flat, meta, *carry = pl.pallas_call(
            lambda *refs: attention_kernel(*refs, carried=len(carry)),
            out_shape=(
                half_shape,
                half_shape,
                jax.ShapeDtypeStruct((seq * heads, 2 * HEAD_DIM), bf16),
                jax.ShapeDtypeStruct((heads, seq), f32),
                jax.ShapeDtypeStruct((seq, LANES), bf16),
                *(jax.ShapeDtypeStruct(array.shape, array.dtype) for array in carry),
            ),
            in_specs=[hbm_spec()] * (13 + len(carry)),
            out_specs=(full_spec(),) * (5 + len(carry)),
            scratch_shapes=[
                pltpu.VMEM((seq, width), bf16),
                pltpu.VMEM((1, width), f32),
                pltpu.VMEM((heads, width), bf16),
                pltpu.VMEM((seq, heads, length), f32),
                pltpu.SMEM((seq,), jnp.int32),
                pltpu.SMEM((heads if heads > 1 else 8,), f32),
                pltpu.VMEM(route_ids.shape[::-1], jnp.int32),
                pltpu.VMEM(route_ids.shape[::-1], f32),
                pltpu.VMEM((width, column), bf16),
                pltpu.VMEM((width, column), bf16),
                pltpu.VMEM((width, column), bf16),
                pltpu.VMEM((column, width), bf16),
                pltpu.VMEM((seq, rows, 2 * HEAD_DIM), bf16),
                pltpu.VMEM((seq * heads, 2 * HEAD_DIM), f32),
                pltpu.VMEM((seq * heads, 2 * HEAD_DIM), f32),
                pltpu.VMEM((seq * heads, 2 * HEAD_DIM), f32),
                pltpu.VMEM((seq * length // LANES * heads, LANES * heads), f32),
                pltpu.VMEM((seq, 2 * heads, rows // 2), f32),
                pltpu.VMEM((seq, 2 * heads, rows // 2), f32),
                pltpu.VMEM((LANES, seq), f32),
                pltpu.SemaphoreType.DMA((12,)),
                pltpu.SemaphoreType.DMA((seq,)),
                pltpu.SemaphoreType.DMA((len(carry),)),
            ],
            compiler_params=pltpu.CompilerParams(vmem_limit_bytes=28 << 20),
            name="attention",
        )(
            *(
                pltpu.with_memory_space_constraint(array, pltpu.HBM)
                for array in (
                    tokens,
                    norm_attn.reshape(1, width),
                    w_forget.T,
                    cache_cum,
                    lengths,
                    b_forget if heads > 1 else jnp.pad(b_forget, (0, 7)),
                    route_ids.T,
                    route_weight.T,
                    w_query,
                    w_key,
                    w_value,
                    w_output,
                    cache_kv.reshape(seq, rows, 2 * HEAD_DIM),
                    *carry,
                )
            ),
        )
        arrived = [
            lax.ppermute(
                other if k % CORES else mine, TENSOR, [(i, i ^ k) for i in range(tensor)]
            )
            for k in range(1, tensor)
        ]
        half = parts * part + LANES
        packed, residual = pl.pallas_call(
            lambda *refs: residual_kernel(*refs, groups=tensor),
            out_shape=(
                jax.ShapeDtypeStruct((groups, seq, half), bf16),
                jax.ShapeDtypeStruct((seq, part), bf16),
            ),
            in_specs=[full_spec()] * (tensor + 2),
            out_specs=(full_spec(),) * 2,
            compiler_params=pltpu.CompilerParams(vmem_limit_bytes=4 << 20),
            name="residual",
        )(mine, *arrived, tokens, meta)
        near = lax.all_to_all(packed, "ep", split_axis=0, concat_axis=0, tiled=True)
        near = near.reshape(groups * seq, half)
        far = lax.ppermute(near, TENSOR, [(i, i ^ 1) for i in range(tensor)])
        keep, send = pl.pallas_call(
            lambda *refs: expert_kernel(*refs, top_count=route_ids.shape[1], seq=seq),
            out_shape=(
                jax.ShapeDtypeStruct((groups, parts, seq, part), f32),
                jax.ShapeDtypeStruct((groups, parts, seq, part), bf16),
            ),
            in_specs=[full_spec()] * 9,
            out_specs=(full_spec(),) * 2,
            scratch_shapes=[pltpu.VMEM((groups * seq, width), bf16)],
            compiler_params=pltpu.CompilerParams(vmem_limit_bytes=8 << 20),
            name="experts",
        )(
            near,
            far,
            norm_ffn.reshape(1, width),
            *carry,
        )
        swapped = lax.ppermute(send, TENSOR, [(i, i ^ 1) for i in range(tensor)])
        chip = (keep + swapped.astype(f32)).astype(bf16)
        pieces = lax.all_to_all(
            chip.reshape(groups * parts, seq, part),
            ("ep", "ty"),
            split_axis=0,
            concat_axis=0,
            tiled=True,
        )
        output = (residual.astype(f32) + jnp.sum(pieces.astype(f32), axis=0)).astype(bf16)
        return output, kv_flat.reshape(seq, heads, 2 * HEAD_DIM), cum_flat.T

    in_specs = (
        P("ep", None),
        P("ep"),
        P("ep", None, TENSOR, None),
        P("ep", TENSOR, None),
        P(),
        P(None, TENSOR),
        P(None, TENSOR),
        P(None, TENSOR),
        P(None, TENSOR),
        P(TENSOR),
        P(TENSOR, None),
        P(),
        P(None, TENSOR),
        P(None, TENSOR),
        P(TENSOR, None),
        P("ep", None, TENSOR),
        P("ep", None, TENSOR),
        P("ep", TENSOR, None),
        P("ep", None),
        P("ep", None),
    )
    out_specs = (P("ep", TENSOR), P("ep", TENSOR, None), P("ep", TENSOR))
    return jax.shard_map(shards, mesh=fine, in_specs=in_specs, out_specs=out_specs, check_vma=False)
```

```python
import jax
import jax.numpy as jnp
from jax import lax
from jax.experimental import pallas as pl
from jax.experimental.pallas import tpu as pltpu
from jax.sharding import Mesh, PartitionSpec as P

HEAD_DIM = 64
CORES = 2
LANES = 128
EPSILON = 1e-06
HUGE = 1 << 30
BATCH = 4
EARLY = 2
AFTER = 4
LATER = 6
TENSOR = ("ty", "tc")

f32 = jnp.float32
bf16 = jnp.bfloat16

NT = (((1,), (1,)), ((), ()))


def field(count):
    return -(-count // 8) * 8


def full_spec():
    return pl.BlockSpec(memory_space=pltpu.VMEM)


def hbm_spec():
    return pl.BlockSpec(memory_space=pltpu.HBM)


def smem_spec():
    return pl.BlockSpec(memory_space=pltpu.SMEM)


def attention_kernel(
    tokens_in,
    norm_in,
    w_forget_in,
    cum_in,
    lengths_in,
    b_forget_in,
    ids_in,
    route_in,
    w_query,
    w_key,
    w_value,
    w_output,
    cache,
    *refs,
    carried,
):
    carry_in, refs = refs[:carried], refs[carried:]
    mine_out, other_out, kv_out, cum_out, meta_out = refs[:5]
    carry_out, refs = refs[5 : 5 + carried], refs[5 + carried :]
    (
        kv_stage,
        cum_stage,
        tokens,
        norm_attn,
        w_forget,
        cum,
        lengths,
        b_forget,
        ids,
        route,
        wq_buf,
        wk_buf,
        wv_buf,
        wo_buf,
        cache_buf,
        q_rows,
        kv_rows,
        att_rows,
        bias_buf,
        shift_buf,
        score_buf,
        meta_rows,
        sem_w,
        sem_c,
        sem_n,
        sem_o,
    ) = refs
    seq, width = tokens.shape
    heads, length = cum.shape[1:]
    half_rows = cache.shape[1] // 2
    half_len = length // 2
    tiles = half_len // LANES
    span = LANES * heads
    pair = 2 * heads
    parts, _, part = mine_out.shape

    moves = (
        (tokens_in, tokens),
        (norm_in, norm_attn),
        (w_forget_in, w_forget),
        (lengths_in, lengths),
        (b_forget_in, b_forget),
        (ids_in, ids),
        (route_in, route),
        (cum_in, cum),
        (w_query, wq_buf),
        (w_key, wk_buf),
        (w_value, wv_buf),
        (w_output, wo_buf),
    )
    w_copies = [
        pltpu.make_async_copy(src, dst, sem_w.at[i]) for i, (src, dst) in enumerate(moves)
    ]
    c_copies = [
        pltpu.make_async_copy(cache.at[s], cache_buf.at[s], sem_c.at[s]) for s in range(seq)
    ]
    n_copies = [
        pltpu.make_async_copy(src, dst, sem_n.at[i])
        for i, (src, dst) in enumerate(zip(carry_in, carry_out))
    ]
    o_copies = [
        pltpu.make_async_copy(kv_stage, kv_out, sem_o.at[0]),
        pltpu.make_async_copy(cum_stage, cum_out, sem_o.at[1]),
    ]
    queue = [*c_copies[:BATCH], *w_copies[9:11], *c_copies[BATCH:], w_copies[11], *n_copies]

    def launch(count):
        for copy in queue[:count]:
            copy.start()
        del queue[:count]

    for copy in w_copies[:9]:
        copy.start()
    launch(EARLY)

    sub = lax.broadcasted_iota(jnp.int32, (LANES, span), 0) * heads
    lane = lax.broadcasted_iota(jnp.int32, (LANES, span), 1)
    spread = ((lane >= sub) & (lane < sub + heads)).astype(f32).astype(bf16)
    row_id = lax.broadcasted_iota(jnp.int32, (pair, half_rows), 0)
    col_id = lax.broadcasted_iota(jnp.int32, (pair, half_rows), 1)
    place = jnp.where(
        lax.rem(row_id, heads) == lax.rem(col_id, heads),
        col_id + jnp.where(row_id >= heads, half_rows, 0),
        HUGE,
    )
    seq_lane = lax.broadcasted_iota(jnp.int32, (heads, seq), 1)
    pos_lane = lax.broadcasted_iota(jnp.int32, (heads, length), 1)
    head_row = lax.broadcasted_iota(jnp.int32, (heads, 1), 0)

    for copy in w_copies[:7]:
        copy.wait()
    launch(AFTER)
    wide = tokens[...].astype(f32)
    scale = lax.rsqrt(jnp.mean(wide * wide, axis=1, keepdims=True) + EPSILON)
    normed = (wide * scale * norm_attn[...]).astype(bf16)
    gate = lax.dot_general(w_forget[...], normed, NT, preferred_element_type=f32)
    for h in range(heads):
        gate = gate + jnp.where(head_row == h, b_forget[h], 0.0)
    forget_log = jnp.minimum(gate, 0.0) - jnp.log1p(jnp.exp(-jnp.abs(gate)))

    top_count = ids.shape[0]
    stride = field(top_count)
    meta_rows[...] = jnp.zeros_like(meta_rows)
    high = route[...].astype(bf16).astype(f32)
    middle = (route[...] - high).astype(bf16).astype(f32)
    for i, value in enumerate((ids[...].astype(f32), high, middle, route[...] - high - middle)):
        meta_rows[i * stride : i * stride + top_count, :] = value
    same = lax.broadcasted_iota(jnp.int32, (seq, seq), 0) == lax.broadcasted_iota(
        jnp.int32, (seq, seq), 1
    )
    meta_out[...] = lax.dot_general(
        same.astype(f32).astype(bf16),
        meta_rows[...].astype(bf16),
        NT,
        preferred_element_type=f32,
    ).astype(bf16)

    w_copies[8].wait()
    launch(LATER)
    query = jnp.dot(normed, wq_buf[...], preferred_element_type=f32).astype(bf16).astype(f32)
    for h in range(heads):
        q_rows[pl.ds(h, seq, stride=heads), :] = jnp.concatenate(
            [
                query[:, h * HEAD_DIM : (h + 1) * HEAD_DIM] * HEAD_DIM ** (-0.5),
                jnp.zeros((seq, HEAD_DIM), f32),
            ],
            axis=1,
        )

    def project():
        w_copies[9].wait()
        w_copies[10].wait()
        key = jnp.dot(normed, wk_buf[...], preferred_element_type=f32).astype(bf16).astype(f32)
        value = jnp.dot(normed, wv_buf[...], preferred_element_type=f32).astype(bf16).astype(f32)
        for h in range(heads):
            cut = slice(h * HEAD_DIM, (h + 1) * HEAD_DIM)
            kv_rows[pl.ds(h, seq, stride=heads), :] = jnp.concatenate(
                [key[:, cut], value[:, cut]], axis=1
            )
        kv_stage[...] = kv_rows[...].astype(bf16)
        o_copies[0].start()

    w_copies[7].wait()
    pieces = []
    for s in range(seq):
        rows = cum[s]
        for j in range(tiles):
            pieces.append(rows[:, j * LANES : (j + 1) * LANES])
            pieces.append(rows[:, half_len + j * LANES : half_len + (j + 1) * LANES])
    stacked = jnp.concatenate(pieces, axis=0)
    hi = stacked.astype(bf16)
    rest = stacked - hi.astype(f32)
    mid = rest.astype(bf16)
    low = (rest - mid.astype(f32)).astype(bf16)
    bias_buf[...] = (
        jnp.dot(hi, spread, preferred_element_type=f32)
        + jnp.dot(mid, spread, preferred_element_type=f32)
        + jnp.dot(low, spread, preferred_element_type=f32)
    )
    cum_all = jnp.zeros((heads, seq), f32)
    for s in range(seq):
        limit = lengths[s]
        last = jnp.sum(jnp.where(pos_lane == limit - 1, cum[s], 0.0), axis=1, keepdims=True)
        cum_new = last + forget_log[:, s : s + 1]
        cum_all = jnp.where(seq_lane == s, cum_new, cum_all)
        cum_two = jnp.concatenate([cum_new, cum_new], axis=0)
        base = s * tiles * pair
        bias = jnp.concatenate(
            [bias_buf[base + j * pair : base + (j + 1) * pair, :] for j in range(tiles)], axis=1
        )
        shift_buf[s] = jnp.where(place < limit * heads, cum_two - bias, -jnp.inf)
    cum_stage[...] = cum_all
    o_copies[1].start()

    def rows_of(s):
        return jnp.concatenate([cache_buf[s, :half_rows, :], cache_buf[s, half_rows:, :]], axis=1)

    def score(s):
        q_s = q_rows[s * heads : (s + 1) * heads, :]
        blank = jnp.zeros_like(q_s)
        lhs = jnp.concatenate(
            [jnp.concatenate([q_s, blank], axis=1), jnp.concatenate([blank, q_s], axis=1)], axis=0
        ).astype(bf16)
        score_buf[s] = lax.dot_general(lhs, rows_of(s), NT, preferred_element_type=f32)

    def attend(s):
        here = slice(s * heads, (s + 1) * heads)
        kv_s = kv_rows[here, :]
        own = jnp.sum(q_rows[here, :] * kv_s, axis=1, keepdims=True)
        scores = score_buf[s] + shift_buf[s]
        top = jnp.max(scores, axis=1, keepdims=True)
        top = jnp.maximum(jnp.maximum(top[:heads], top[heads:]), own)
        weights = jnp.exp(scores - jnp.concatenate([top, top], axis=0))
        weight_own = jnp.exp(own - top)
        total = jnp.sum(weights, axis=1, keepdims=True)
        inverse = 1.0 / (total[:heads] + total[heads:] + weight_own)
        probs = (weights * jnp.concatenate([inverse, inverse], axis=0)).astype(bf16)
        prob_own = (weight_own * inverse).astype(bf16).astype(f32)
        mixed = jnp.dot(probs, rows_of(s), preferred_element_type=f32)
        att_rows[here, :] = mixed[:heads, :LANES] + mixed[heads:, LANES:] + prob_own * kv_s

    for start in range(0, seq + BATCH, BATCH):
        if start < seq:
            for s in range(start, start + BATCH):
                c_copies[s].wait()
            launch(BATCH if start + BATCH < seq else len(queue))
            for s in range(start, start + BATCH):
                score(s)
        if start == 0:
            project()
        if start:
            for s in range(start - BATCH, start):
                attend(s)

    attended = jnp.concatenate(
        [att_rows[pl.ds(h, seq, stride=heads), :][:, HEAD_DIM:] for h in range(heads)], axis=1
    ).astype(bf16)
    w_copies[11].wait()
    core = lax.rem(lax.axis_index(TENSOR), CORES)
    for y in range(parts):
        here = pl.ds(pl.multiple_of((y * CORES + core) * part, part), part)
        mine_out[y] = jnp.dot(attended, wo_buf[:, here], preferred_element_type=f32).astype(bf16)
        there = pl.ds(pl.multiple_of((y * CORES + 1 - core) * part, part), part)
        other_out[y] = jnp.dot(attended, wo_buf[:, there], preferred_element_type=f32).astype(bf16)
    for copy in n_copies + o_copies:
        copy.wait()


def residual_kernel(*refs, groups):
    mine = refs[0]
    arrived = refs[1 : 1 + groups - 1]
    tokens, meta, packed_out, residual_out = refs[groups:]
    parts, _, part = mine.shape
    place = lax.axis_index(TENSOR)
    core = lax.rem(place, CORES)
    for y in range(parts):
        here = pl.ds(pl.multiple_of((y * CORES + core) * part, part), part)
        total = mine[y].astype(f32)
        for ref in arrived:
            total = total + ref[y].astype(f32)
        rounded = (tokens[:, here].astype(f32) + total).astype(bf16)
        for e in range(packed_out.shape[0]):
            packed_out[e, :, y * part : (y + 1) * part] = rounded

        @pl.when(place == y * CORES + core)
        def _():
            residual_out[...] = rounded

    for e in range(packed_out.shape[0]):
        packed_out[e, :, parts * part :] = meta[...]


def expert_kernel(
    near,
    far,
    norm_ffn,
    shared_gate,
    shared_up,
    shared_down,
    expert_gate,
    expert_up,
    expert_down,
    keep_out,
    send_out,
    rows_buf,
    *,
    top_count,
    seq,
):
    groups, parts, _, part = keep_out.shape
    row_count = near.shape[0]
    width = rows_buf.shape[1]
    core = lax.rem(lax.axis_index(TENSOR), CORES)
    group = lax.axis_index("ep")
    experts = expert_gate.shape[0]
    hidden = expert_gate.shape[2]

    squares = jnp.zeros((row_count, 1), f32)
    for ref in (near, far):
        for y in range(parts):
            piece = ref[:, y * part : (y + 1) * part].astype(f32)
            squares = squares + jnp.sum(piece * piece, axis=1, keepdims=True)
    scale = lax.rsqrt(squares * (1.0 / width) + EPSILON)
    for ref, side in ((near, core), (far, 1 - core)):
        for y in range(parts):
            here = pl.ds(pl.multiple_of((y * CORES + side) * part, part), part)
            piece = ref[:, y * part : (y + 1) * part].astype(f32)
            rows_buf[:, here] = (piece * scale * norm_ffn[:, here]).astype(bf16)

    meta = near[:, parts * part :].astype(f32)
    ids = meta[:, :top_count]
    stride = field(top_count)
    coef = (
        meta[:, stride : stride + top_count]
        + meta[:, 2 * stride : 2 * stride + top_count]
        + meta[:, 3 * stride : 3 * stride + top_count]
    )
    row_id = lax.broadcasted_iota(jnp.int32, (row_count, 1), 0)
    own = (row_id >= group * seq) & (row_id < (group + 1) * seq)
    rows = rows_buf[...]
    lane_full = hidden % LANES == 0

    def hidden_units(w_gate, w_up, factor):
        if lane_full:
            both = jnp.dot(
                rows, jnp.concatenate([w_gate, w_up], axis=1), preferred_element_type=f32
            )
            gate, up = both[:, :hidden], both[:, hidden:]
        else:
            gate = jnp.dot(rows, w_gate, preferred_element_type=f32)
            up = jnp.dot(rows, w_up, preferred_element_type=f32)
        return (gate / (1.0 + jnp.exp(-gate)) * up * factor).astype(bf16)

    units = []
    for e in range(experts):
        wanted = (group * experts + e).astype(f32)
        factor = jnp.sum(jnp.where(ids == wanted, coef, 0.0), axis=1, keepdims=True)
        units.append(hidden_units(expert_gate[e], expert_up[e], factor))
    units.append(hidden_units(shared_gate[...], shared_up[...], own.astype(f32)))
    if lane_full:
        joined = jnp.concatenate(units, axis=1)

    def down(here):
        blocks = [expert_down[e, :, here] for e in range(experts)] + [shared_down[:, here]]
        if lane_full:
            return jnp.dot(joined, jnp.concatenate(blocks, axis=0), preferred_element_type=f32)
        total = jnp.dot(units[0], blocks[0], preferred_element_type=f32)
        for unit, block in zip(units[1:], blocks[1:]):
            total = total + jnp.dot(unit, block, preferred_element_type=f32)
        return total

    for out, side in ((send_out, 1 - core), (keep_out, core)):
        for y in range(parts):
            here = pl.ds(pl.multiple_of((y * CORES + side) * part, part), part)
            result = down(here)
            for g in range(groups):
                out[g, y] = result[g * seq : (g + 1) * seq].astype(out.dtype)


def solution(mesh):
    groups = mesh.shape["ep"]
    tensor = mesh.shape["tp"]
    parts = tensor // CORES
    fine = Mesh(mesh.devices.reshape(groups, parts, CORES), ("ep", "ty", "tc"))

    def shards(
        tokens,
        lengths,
        cache_kv,
        cache_cum,
        norm_attn,
        w_query,
        w_key,
        w_value,
        w_forget,
        b_forget,
        w_output,
        norm_ffn,
        shared_gate,
        shared_up,
        shared_down,
        expert_gate,
        expert_up,
        expert_down,
        route_ids,
        route_weight,
    ):
        seq, width = tokens.shape
        heads, length = cache_cum.shape[1:]
        part = width // tensor
        rows = length * heads
        column = heads * HEAD_DIM
        half_shape = jax.ShapeDtypeStruct((parts, seq, part), bf16)
        carry = (shared_gate, shared_up, shared_down, expert_gate, expert_up, expert_down)
        mine, other, kv_flat, cum_flat, meta, *carry = pl.pallas_call(
            lambda *refs: attention_kernel(*refs, carried=len(carry)),
            out_shape=(
                half_shape,
                half_shape,
                jax.ShapeDtypeStruct((seq * heads, 2 * HEAD_DIM), bf16),
                jax.ShapeDtypeStruct((heads, seq), f32),
                jax.ShapeDtypeStruct((seq, LANES), bf16),
                *(jax.ShapeDtypeStruct(array.shape, array.dtype) for array in carry),
            ),
            in_specs=[hbm_spec()] * (13 + len(carry)),
            out_specs=(
                *[full_spec()] * 2,
                *[hbm_spec()] * 2,
                *[full_spec()] * (1 + len(carry)),
            ),
            scratch_shapes=[
                pltpu.VMEM((seq * heads, 2 * HEAD_DIM), bf16),
                pltpu.VMEM((heads, seq), f32),
                pltpu.VMEM((seq, width), bf16),
                pltpu.VMEM((1, width), f32),
                pltpu.VMEM((heads, width), bf16),
                pltpu.VMEM((seq, heads, length), f32),
                pltpu.SMEM((seq,), jnp.int32),
                pltpu.SMEM((heads if heads > 1 else 8,), f32),
                pltpu.VMEM(route_ids.shape[::-1], jnp.int32),
                pltpu.VMEM(route_ids.shape[::-1], f32),
                pltpu.VMEM((width, column), bf16),
                pltpu.VMEM((width, column), bf16),
                pltpu.VMEM((width, column), bf16),
                pltpu.VMEM((column, width), bf16),
                pltpu.VMEM((seq, rows, 2 * HEAD_DIM), bf16),
                pltpu.VMEM((seq * heads, 2 * HEAD_DIM), f32),
                pltpu.VMEM((seq * heads, 2 * HEAD_DIM), f32),
                pltpu.VMEM((seq * heads, 2 * HEAD_DIM), f32),
                pltpu.VMEM((seq * length // LANES * heads, LANES * heads), f32),
                pltpu.VMEM((seq, 2 * heads, rows // 2), f32),
                pltpu.VMEM((seq, 2 * heads, rows // 2), f32),
                pltpu.VMEM((LANES, seq), f32),
                pltpu.SemaphoreType.DMA((12,)),
                pltpu.SemaphoreType.DMA((seq,)),
                pltpu.SemaphoreType.DMA((len(carry),)),
                pltpu.SemaphoreType.DMA((2,)),
            ],
            compiler_params=pltpu.CompilerParams(vmem_limit_bytes=28 << 20),
            name="attention",
        )(
            *(
                pltpu.with_memory_space_constraint(array, pltpu.HBM)
                for array in (
                    tokens,
                    norm_attn.reshape(1, width),
                    w_forget.T,
                    cache_cum,
                    lengths,
                    b_forget if heads > 1 else jnp.pad(b_forget, (0, 7)),
                    route_ids.T,
                    route_weight.T,
                    w_query,
                    w_key,
                    w_value,
                    w_output,
                    cache_kv.reshape(seq, rows, 2 * HEAD_DIM),
                    *carry,
                )
            ),
        )
        arrived = [
            lax.ppermute(
                other if k % CORES else mine, TENSOR, [(i, i ^ k) for i in range(tensor)]
            )
            for k in range(1, tensor)
        ]
        half = parts * part + LANES
        packed, residual = pl.pallas_call(
            lambda *refs: residual_kernel(*refs, groups=tensor),
            out_shape=(
                jax.ShapeDtypeStruct((groups, seq, half), bf16),
                jax.ShapeDtypeStruct((seq, part), bf16),
            ),
            in_specs=[full_spec()] * (tensor + 2),
            out_specs=(full_spec(),) * 2,
            compiler_params=pltpu.CompilerParams(vmem_limit_bytes=4 << 20),
            name="residual",
        )(mine, *arrived, tokens, meta)
        near = lax.all_to_all(packed, "ep", split_axis=0, concat_axis=0, tiled=True)
        near = near.reshape(groups * seq, half)
        far = lax.ppermute(near, TENSOR, [(i, i ^ 1) for i in range(tensor)])
        keep, send = pl.pallas_call(
            lambda *refs: expert_kernel(*refs, top_count=route_ids.shape[1], seq=seq),
            out_shape=(
                jax.ShapeDtypeStruct((groups, parts, seq, part), f32),
                jax.ShapeDtypeStruct((groups, parts, seq, part), bf16),
            ),
            in_specs=[full_spec()] * 9,
            out_specs=(full_spec(),) * 2,
            scratch_shapes=[pltpu.VMEM((groups * seq, width), bf16)],
            compiler_params=pltpu.CompilerParams(vmem_limit_bytes=8 << 20),
            name="experts",
        )(
            near,
            far,
            norm_ffn.reshape(1, width),
            *carry,
        )
        swapped = lax.ppermute(send, TENSOR, [(i, i ^ 1) for i in range(tensor)])
        chip = (keep + swapped.astype(f32)).astype(bf16)
        pieces = lax.all_to_all(
            chip.reshape(groups * parts, seq, part),
            ("ep", "ty"),
            split_axis=0,
            concat_axis=0,
            tiled=True,
        )
        output = (residual.astype(f32) + jnp.sum(pieces.astype(f32), axis=0)).astype(bf16)
        return output, kv_flat.reshape(seq, heads, 2 * HEAD_DIM), cum_flat.T

    in_specs = (
        P("ep", None),
        P("ep"),
        P("ep", None, TENSOR, None),
        P("ep", TENSOR, None),
        P(),
        P(None, TENSOR),
        P(None, TENSOR),
        P(None, TENSOR),
        P(None, TENSOR),
        P(TENSOR),
        P(TENSOR, None),
        P(),
        P(None, TENSOR),
        P(None, TENSOR),
        P(TENSOR, None),
        P("ep", None, TENSOR),
        P("ep", None, TENSOR),
        P("ep", TENSOR, None),
        P("ep", None),
        P("ep", None),
    )
    out_specs = (P("ep", TENSOR), P("ep", TENSOR, None), P("ep", TENSOR))
    return jax.shard_map(shards, mesh=fine, in_specs=in_specs, out_specs=out_specs, check_vma=False)
```

```python
import jax
import jax.numpy as jnp
from jax import lax
from jax.experimental import pallas as pl
from jax.experimental.pallas import tpu as pltpu
from jax.sharding import Mesh, PartitionSpec as P

HEAD_DIM = 64
CORES = 2
LANES = 128
EPSILON = 1e-06
HUGE = 1 << 30
SHARES = (0, 4, 10)
EARLY = 6
AFTER = 4
LATER = 8
TENSOR = ("ty", "tc")

f32 = jnp.float32
bf16 = jnp.bfloat16

NT = (((1,), (1,)), ((), ()))


def field(count):
    return -(-count // 8) * 8


def full_spec():
    return pl.BlockSpec(memory_space=pltpu.VMEM)


def hbm_spec():
    return pl.BlockSpec(memory_space=pltpu.HBM)


def smem_spec():
    return pl.BlockSpec(memory_space=pltpu.SMEM)


def attention_kernel(
    tokens_in,
    norm_in,
    w_forget_in,
    cum_in,
    lengths_in,
    b_forget_in,
    ids_in,
    route_in,
    w_query,
    w_key,
    w_value,
    w_output,
    cache,
    *refs,
    carried,
):
    carry_in, refs = refs[:carried], refs[carried:]
    mine_out, other_out, kv_out, cum_out, meta_out = refs[:5]
    carry_out, refs = refs[5 : 5 + carried], refs[5 + carried :]
    (
        kv_stage,
        cum_stage,
        tokens,
        norm_attn,
        w_forget,
        cum,
        lengths,
        b_forget,
        ids,
        route,
        wq_buf,
        wk_buf,
        wv_buf,
        wo_buf,
        cache_buf,
        q_rows,
        kv_rows,
        att_rows,
        bias_buf,
        shift_buf,
        score_buf,
        meta_rows,
        sem_w,
        sem_c,
        sem_n,
        sem_o,
    ) = refs
    seq, width = tokens.shape
    heads, length = cum.shape[1:]
    half_rows = cache.shape[1] // 2
    half_len = length // 2
    tiles = half_len // LANES
    span = LANES * heads
    pair = 2 * heads
    parts, _, part = mine_out.shape

    moves = (
        (tokens_in, tokens),
        (norm_in, norm_attn),
        (w_forget_in, w_forget),
        (lengths_in, lengths),
        (b_forget_in, b_forget),
        (ids_in, ids),
        (route_in, route),
        (cum_in, cum),
        (w_query, wq_buf),
        (w_key, wk_buf),
        (w_value, wv_buf),
        (w_output, wo_buf),
    )
    w_copies = [
        pltpu.make_async_copy(src, dst, sem_w.at[i]) for i, (src, dst) in enumerate(moves)
    ]
    c_copies = [
        pltpu.make_async_copy(cache.at[s], cache_buf.at[s], sem_c.at[s]) for s in range(seq)
    ]
    n_copies = [
        pltpu.make_async_copy(src, dst, sem_n.at[i])
        for i, (src, dst) in enumerate(zip(carry_in, carry_out))
    ]
    o_copies = [
        pltpu.make_async_copy(kv_stage, kv_out, sem_o.at[0]),
        pltpu.make_async_copy(cum_stage, cum_out, sem_o.at[1]),
    ]
    first = seq * SHARES[1] // 16
    queue = [*c_copies[:first], *w_copies[9:11], *c_copies[first:], w_copies[11], *n_copies]

    def launch(count):
        for copy in queue[:count]:
            copy.start()
        del queue[:count]

    for copy in w_copies[:9]:
        copy.start()
    launch(EARLY)

    sub = lax.broadcasted_iota(jnp.int32, (LANES, span), 0) * heads
    lane = lax.broadcasted_iota(jnp.int32, (LANES, span), 1)
    spread = ((lane >= sub) & (lane < sub + heads)).astype(f32).astype(bf16)
    row_id = lax.broadcasted_iota(jnp.int32, (pair, half_rows), 0)
    col_id = lax.broadcasted_iota(jnp.int32, (pair, half_rows), 1)
    place = jnp.where(
        lax.rem(row_id, heads) == lax.rem(col_id, heads),
        col_id + jnp.where(row_id >= heads, half_rows, 0),
        HUGE,
    )
    seq_lane = lax.broadcasted_iota(jnp.int32, (heads, seq), 1)
    pos_lane = lax.broadcasted_iota(jnp.int32, (heads, length), 1)
    head_row = lax.broadcasted_iota(jnp.int32, (heads, 1), 0)

    for copy in w_copies[:7]:
        copy.wait()
    launch(AFTER)
    wide = tokens[...].astype(f32)
    scale = lax.rsqrt(jnp.mean(wide * wide, axis=1, keepdims=True) + EPSILON)
    normed = (wide * scale * norm_attn[...]).astype(bf16)
    gate = lax.dot_general(w_forget[...], normed, NT, preferred_element_type=f32)
    for h in range(heads):
        gate = gate + jnp.where(head_row == h, b_forget[h], 0.0)
    forget_log = jnp.minimum(gate, 0.0) - jnp.log1p(jnp.exp(-jnp.abs(gate)))

    top_count = ids.shape[0]
    stride = field(top_count)
    meta_rows[...] = jnp.zeros_like(meta_rows)
    high = route[...].astype(bf16).astype(f32)
    middle = (route[...] - high).astype(bf16).astype(f32)
    for i, value in enumerate((ids[...].astype(f32), high, middle, route[...] - high - middle)):
        meta_rows[i * stride : i * stride + top_count, :] = value
    same = lax.broadcasted_iota(jnp.int32, (seq, seq), 0) == lax.broadcasted_iota(
        jnp.int32, (seq, seq), 1
    )
    meta_out[...] = lax.dot_general(
        same.astype(f32).astype(bf16),
        meta_rows[...].astype(bf16),
        NT,
        preferred_element_type=f32,
    ).astype(bf16)

    w_copies[7].wait()
    pieces = []
    for s in range(seq):
        rows = cum[s]
        for j in range(tiles):
            pieces.append(rows[:, j * LANES : (j + 1) * LANES])
            pieces.append(rows[:, half_len + j * LANES : half_len + (j + 1) * LANES])
    stacked = jnp.concatenate(pieces, axis=0)
    hi = stacked.astype(bf16)
    rest = stacked - hi.astype(f32)
    mid = rest.astype(bf16)
    low = (rest - mid.astype(f32)).astype(bf16)
    bias_buf[...] = (
        jnp.dot(hi, spread, preferred_element_type=f32)
        + jnp.dot(mid, spread, preferred_element_type=f32)
        + jnp.dot(low, spread, preferred_element_type=f32)
    )
    cum_all = jnp.zeros((heads, seq), f32)
    for s in range(seq):
        limit = lengths[s]
        last = jnp.sum(jnp.where(pos_lane == limit - 1, cum[s], 0.0), axis=1, keepdims=True)
        cum_new = last + forget_log[:, s : s + 1]
        cum_all = jnp.where(seq_lane == s, cum_new, cum_all)
        cum_two = jnp.concatenate([cum_new, cum_new], axis=0)
        base = s * tiles * pair
        bias = jnp.concatenate(
            [bias_buf[base + j * pair : base + (j + 1) * pair, :] for j in range(tiles)], axis=1
        )
        shift_buf[s] = jnp.where(place < limit * heads, cum_two - bias, -jnp.inf)
    cum_stage[...] = cum_all
    o_copies[1].start()

    w_copies[8].wait()
    launch(LATER)
    query = jnp.dot(normed, wq_buf[...], preferred_element_type=f32).astype(bf16).astype(f32)
    for h in range(heads):
        q_rows[pl.ds(h, seq, stride=heads), :] = jnp.concatenate(
            [
                query[:, h * HEAD_DIM : (h + 1) * HEAD_DIM] * HEAD_DIM ** (-0.5),
                jnp.zeros((seq, HEAD_DIM), f32),
            ],
            axis=1,
        )

    def project():
        w_copies[9].wait()
        w_copies[10].wait()
        key = jnp.dot(normed, wk_buf[...], preferred_element_type=f32).astype(bf16).astype(f32)
        value = jnp.dot(normed, wv_buf[...], preferred_element_type=f32).astype(bf16).astype(f32)
        for h in range(heads):
            cut = slice(h * HEAD_DIM, (h + 1) * HEAD_DIM)
            kv_rows[pl.ds(h, seq, stride=heads), :] = jnp.concatenate(
                [key[:, cut], value[:, cut]], axis=1
            )
        kv_stage[...] = kv_rows[...].astype(bf16)
        o_copies[0].start()

    def rows_of(s):
        return jnp.concatenate([cache_buf[s, :half_rows, :], cache_buf[s, half_rows:, :]], axis=1)

    def score(s):
        q_s = q_rows[s * heads : (s + 1) * heads, :]
        blank = jnp.zeros_like(q_s)
        lhs = jnp.concatenate(
            [jnp.concatenate([q_s, blank], axis=1), jnp.concatenate([blank, q_s], axis=1)], axis=0
        ).astype(bf16)
        score_buf[s] = lax.dot_general(lhs, rows_of(s), NT, preferred_element_type=f32)

    def attend(s):
        here = slice(s * heads, (s + 1) * heads)
        kv_s = kv_rows[here, :]
        own = jnp.sum(q_rows[here, :] * kv_s, axis=1, keepdims=True)
        scores = score_buf[s] + shift_buf[s]
        top = jnp.max(scores, axis=1, keepdims=True)
        top = jnp.maximum(jnp.maximum(top[:heads], top[heads:]), own)
        weights = jnp.exp(scores - jnp.concatenate([top, top], axis=0))
        weight_own = jnp.exp(own - top)
        total = jnp.sum(weights, axis=1, keepdims=True)
        inverse = 1.0 / (total[:heads] + total[heads:] + weight_own)
        probs = (weights * jnp.concatenate([inverse, inverse], axis=0)).astype(bf16)
        prob_own = (weight_own * inverse).astype(bf16).astype(f32)
        mixed = jnp.dot(probs, rows_of(s), preferred_element_type=f32)
        att_rows[here, :] = mixed[:heads, :LANES] + mixed[heads:, LANES:] + prob_own * kv_s

    bounds = [seq * share // 16 for share in SHARES]
    before = 0
    for start, stop in zip(bounds, bounds[1:] + [seq]):
        for s in range(start, stop):
            c_copies[s].wait()
        launch(len(queue))
        for s in range(start, stop):
            score(s)
        if start == 0:
            project()
        for s in range(before, start):
            attend(s)
        before = start
    for s in range(before, seq):
        attend(s)

    attended = jnp.concatenate(
        [att_rows[pl.ds(h, seq, stride=heads), :][:, HEAD_DIM:] for h in range(heads)], axis=1
    ).astype(bf16)
    w_copies[11].wait()
    core = lax.rem(lax.axis_index(TENSOR), CORES)
    for y in range(parts):
        here = pl.ds(pl.multiple_of((y * CORES + core) * part, part), part)
        mine_out[y] = jnp.dot(attended, wo_buf[:, here], preferred_element_type=f32).astype(bf16)
        there = pl.ds(pl.multiple_of((y * CORES + 1 - core) * part, part), part)
        other_out[y] = jnp.dot(attended, wo_buf[:, there], preferred_element_type=f32).astype(bf16)
    for copy in n_copies + o_copies:
        copy.wait()


def residual_kernel(*refs, groups):
    mine = refs[0]
    arrived = refs[1 : 1 + groups - 1]
    tokens, meta, packed_out, residual_out = refs[groups:]
    parts, _, part = mine.shape
    place = lax.axis_index(TENSOR)
    core = lax.rem(place, CORES)
    for y in range(parts):
        here = pl.ds(pl.multiple_of((y * CORES + core) * part, part), part)
        total = mine[y].astype(f32)
        for ref in arrived:
            total = total + ref[y].astype(f32)
        rounded = (tokens[:, here].astype(f32) + total).astype(bf16)
        for e in range(packed_out.shape[0]):
            packed_out[e, :, y * part : (y + 1) * part] = rounded

        @pl.when(place == y * CORES + core)
        def _():
            residual_out[...] = rounded

    for e in range(packed_out.shape[0]):
        packed_out[e, :, parts * part :] = meta[...]


def half_products(rows, norm_ffn, gates, ups, side, part):
    parts = rows.shape[1] // part
    squares, totals = 0.0, [0.0] * len(gates)
    for y in range(parts):
        here = pl.ds(pl.multiple_of((y * CORES + side) * part, part), part)
        piece = rows[:, y * part : (y + 1) * part].astype(f32)
        squares = squares + jnp.sum(piece * piece, axis=1, keepdims=True)
        gained = (piece * norm_ffn[:, here]).astype(bf16)
        for e, (gate, up) in enumerate(zip(gates, ups)):
            w_gate, w_up = gate[here, :], up[here, :]
            if w_gate.shape[1] % LANES == 0:
                both = jnp.dot(
                    gained, jnp.concatenate([w_gate, w_up], axis=1), preferred_element_type=f32
                )
            else:
                both = jnp.concatenate(
                    [
                        jnp.dot(gained, w_gate, preferred_element_type=f32),
                        jnp.dot(gained, w_up, preferred_element_type=f32),
                    ],
                    axis=1,
                )
            totals[e] = totals[e] + both
    return squares, totals


def near_kernel(
    near,
    norm_ffn,
    shared_gate,
    shared_up,
    expert_gate,
    expert_up,
    product_out,
    square_out,
    factor_out,
    *,
    top_count,
    seq,
    part,
):
    row_count = near.shape[0]
    experts = expert_gate.shape[0]
    half = near.shape[1] - LANES
    core = lax.rem(lax.axis_index(TENSOR), CORES)
    group = lax.axis_index("ep")
    squares, totals = half_products(
        near.at[:, :half],
        norm_ffn,
        [expert_gate.at[e] for e in range(experts)] + [shared_gate],
        [expert_up.at[e] for e in range(experts)] + [shared_up],
        core,
        part,
    )
    square_out[...] = squares
    for e, total in enumerate(totals):
        product_out[e] = total
    meta = near[:, half:].astype(f32)
    ids = meta[:, :top_count]
    stride = field(top_count)
    coef = (
        meta[:, stride : stride + top_count]
        + meta[:, 2 * stride : 2 * stride + top_count]
        + meta[:, 3 * stride : 3 * stride + top_count]
    )
    for e in range(experts):
        wanted = (group * experts + e).astype(f32)
        factor_out[e] = jnp.sum(jnp.where(ids == wanted, coef, 0.0), axis=1, keepdims=True)
    row_id = lax.broadcasted_iota(jnp.int32, (row_count, 1), 0)
    own = (row_id >= group * seq) & (row_id < (group + 1) * seq)
    factor_out[experts] = own.astype(f32)


def down_products(units, blocks):
    hidden = units[0].shape[1]
    if hidden % LANES == 0:
        return jnp.dot(
            jnp.concatenate(units, axis=1),
            jnp.concatenate(blocks, axis=0),
            preferred_element_type=f32,
        )
    total = jnp.dot(units[0], blocks[0], preferred_element_type=f32)
    for unit, block in zip(units[1:], blocks[1:]):
        total = total + jnp.dot(unit, block, preferred_element_type=f32)
    return total


def down_half(units, shared_down, expert_down, out, side):
    groups, parts, seq, part = out.shape
    for y in range(parts):
        here = pl.ds(pl.multiple_of((y * CORES + side) * part, part), part)
        blocks = [expert_down[e, :, here] for e in range(expert_down.shape[0])]
        result = down_products(units, blocks + [shared_down[:, here]])
        for g in range(groups):
            out[g, y] = result[g * seq : (g + 1) * seq].astype(out.dtype)


def far_kernel(
    far,
    products,
    near_squares,
    factors,
    norm_ffn,
    shared_gate,
    shared_up,
    shared_down,
    expert_gate,
    expert_up,
    expert_down,
    send_out,
    unit_out,
    *,
    part,
):
    experts = expert_gate.shape[0]
    hidden = expert_gate.shape[2]
    half = far.shape[1] - LANES
    side = 1 - lax.rem(lax.axis_index(TENSOR), CORES)
    squares, totals = half_products(
        far.at[:, :half],
        norm_ffn,
        [expert_gate.at[e] for e in range(experts)] + [shared_gate],
        [expert_up.at[e] for e in range(experts)] + [shared_up],
        side,
        part,
    )
    width = expert_down.shape[2]
    scale = lax.rsqrt((squares + near_squares[...]) * (1.0 / width) + EPSILON)
    units = []
    for e, total in enumerate(totals):
        both = (total + products[e]) * scale
        gate, up = both[:, :hidden], both[:, hidden:]
        units.append((gate / (1.0 + jnp.exp(-gate)) * up * factors[e]).astype(bf16))
        unit_out[e] = units[e]
    down_half(units, shared_down, expert_down, send_out, side)


def keep_kernel(units, shared_down, expert_down, keep_out):
    core = lax.rem(lax.axis_index(TENSOR), CORES)
    down_half([units[e] for e in range(units.shape[0])], shared_down, expert_down, keep_out, core)


def solution(mesh):
    groups = mesh.shape["ep"]
    tensor = mesh.shape["tp"]
    parts = tensor // CORES
    fine = Mesh(mesh.devices.reshape(groups, parts, CORES), ("ep", "ty", "tc"))

    def shards(
        tokens,
        lengths,
        cache_kv,
        cache_cum,
        norm_attn,
        w_query,
        w_key,
        w_value,
        w_forget,
        b_forget,
        w_output,
        norm_ffn,
        shared_gate,
        shared_up,
        shared_down,
        expert_gate,
        expert_up,
        expert_down,
        route_ids,
        route_weight,
    ):
        seq, width = tokens.shape
        heads, length = cache_cum.shape[1:]
        part = width // tensor
        rows = length * heads
        column = heads * HEAD_DIM
        half_shape = jax.ShapeDtypeStruct((parts, seq, part), bf16)
        carry = (shared_gate, shared_up, shared_down, expert_gate, expert_up, expert_down)
        mine, other, kv_flat, cum_flat, meta, *carry = pl.pallas_call(
            lambda *refs: attention_kernel(*refs, carried=len(carry)),
            out_shape=(
                half_shape,
                half_shape,
                jax.ShapeDtypeStruct((seq * heads, 2 * HEAD_DIM), bf16),
                jax.ShapeDtypeStruct((heads, seq), f32),
                jax.ShapeDtypeStruct((seq, LANES), bf16),
                *(jax.ShapeDtypeStruct(array.shape, array.dtype) for array in carry),
            ),
            in_specs=[hbm_spec()] * (13 + len(carry)),
            out_specs=(
                *[full_spec()] * 2,
                *[hbm_spec()] * 2,
                *[full_spec()] * (1 + len(carry)),
            ),
            scratch_shapes=[
                pltpu.VMEM((seq * heads, 2 * HEAD_DIM), bf16),
                pltpu.VMEM((heads, seq), f32),
                pltpu.VMEM((seq, width), bf16),
                pltpu.VMEM((1, width), f32),
                pltpu.VMEM((heads, width), bf16),
                pltpu.VMEM((seq, heads, length), f32),
                pltpu.SMEM((seq,), jnp.int32),
                pltpu.SMEM((heads if heads > 1 else 8,), f32),
                pltpu.VMEM(route_ids.shape[::-1], jnp.int32),
                pltpu.VMEM(route_ids.shape[::-1], f32),
                pltpu.VMEM((width, column), bf16),
                pltpu.VMEM((width, column), bf16),
                pltpu.VMEM((width, column), bf16),
                pltpu.VMEM((column, width), bf16),
                pltpu.VMEM((seq, rows, 2 * HEAD_DIM), bf16),
                pltpu.VMEM((seq * heads, 2 * HEAD_DIM), f32),
                pltpu.VMEM((seq * heads, 2 * HEAD_DIM), f32),
                pltpu.VMEM((seq * heads, 2 * HEAD_DIM), f32),
                pltpu.VMEM((seq * length // LANES * heads, LANES * heads), f32),
                pltpu.VMEM((seq, 2 * heads, rows // 2), f32),
                pltpu.VMEM((seq, 2 * heads, rows // 2), f32),
                pltpu.VMEM((LANES, seq), f32),
                pltpu.SemaphoreType.DMA((12,)),
                pltpu.SemaphoreType.DMA((seq,)),
                pltpu.SemaphoreType.DMA((len(carry),)),
                pltpu.SemaphoreType.DMA((2,)),
            ],
            compiler_params=pltpu.CompilerParams(vmem_limit_bytes=28 << 20),
            name="attention",
        )(
            *(
                pltpu.with_memory_space_constraint(array, pltpu.HBM)
                for array in (
                    tokens,
                    norm_attn.reshape(1, width),
                    w_forget.T,
                    cache_cum,
                    lengths,
                    b_forget if heads > 1 else jnp.pad(b_forget, (0, 7)),
                    route_ids.T,
                    route_weight.T,
                    w_query,
                    w_key,
                    w_value,
                    w_output,
                    cache_kv.reshape(seq, rows, 2 * HEAD_DIM),
                    *carry,
                )
            ),
        )
        arrived = [
            lax.ppermute(
                other if k % CORES else mine, TENSOR, [(i, i ^ k) for i in range(tensor)]
            )
            for k in range(1, tensor)
        ]
        half = parts * part + LANES
        packed, residual = pl.pallas_call(
            lambda *refs: residual_kernel(*refs, groups=tensor),
            out_shape=(
                jax.ShapeDtypeStruct((groups, seq, half), bf16),
                jax.ShapeDtypeStruct((seq, part), bf16),
            ),
            in_specs=[full_spec()] * (tensor + 2),
            out_specs=(full_spec(),) * 2,
            compiler_params=pltpu.CompilerParams(vmem_limit_bytes=4 << 20),
            name="residual",
        )(mine, *arrived, tokens, meta)
        near = lax.all_to_all(packed, "ep", split_axis=0, concat_axis=0, tiled=True)
        near = near.reshape(groups * seq, half)
        far = lax.ppermute(near, TENSOR, [(i, i ^ 1) for i in range(tensor)])
        experts, _, hidden = expert_gate.shape
        row_count = groups * seq
        gain = norm_ffn.reshape(1, width)
        s_gate, s_up, s_down, e_gate, e_up, e_down = carry
        small = pltpu.CompilerParams(vmem_limit_bytes=8 << 20)
        products, squares, factors = pl.pallas_call(
            lambda *refs: near_kernel(
                *refs, top_count=route_ids.shape[1], seq=seq, part=part
            ),
            out_shape=(
                jax.ShapeDtypeStruct((experts + 1, row_count, 2 * hidden), f32),
                jax.ShapeDtypeStruct((row_count, 1), f32),
                jax.ShapeDtypeStruct((experts + 1, row_count, 1), f32),
            ),
            in_specs=[full_spec()] * 6,
            out_specs=(full_spec(),) * 3,
            compiler_params=small,
            name="near",
        )(near, gain, s_gate, s_up, e_gate, e_up)
        send, units = pl.pallas_call(
            lambda *refs: far_kernel(*refs, part=part),
            out_shape=(
                jax.ShapeDtypeStruct((groups, parts, seq, part), bf16),
                jax.ShapeDtypeStruct((experts + 1, row_count, hidden), bf16),
            ),
            in_specs=[full_spec()] * 11,
            out_specs=(full_spec(),) * 2,
            compiler_params=small,
            name="far",
        )(far, products, squares, factors, gain, *carry)
        swapped = lax.ppermute(send, TENSOR, [(i, i ^ 1) for i in range(tensor)])
        keep = pl.pallas_call(
            keep_kernel,
            out_shape=jax.ShapeDtypeStruct((groups, parts, seq, part), f32),
            in_specs=[full_spec()] * 3,
            out_specs=full_spec(),
            compiler_params=small,
            name="keep",
        )(units, s_down, e_down)
        chip = (keep + swapped.astype(f32)).astype(bf16)
        pieces = lax.all_to_all(
            chip.reshape(groups * parts, seq, part),
            ("ep", "ty"),
            split_axis=0,
            concat_axis=0,
            tiled=True,
        )
        output = (residual.astype(f32) + jnp.sum(pieces.astype(f32), axis=0)).astype(bf16)
        return output, kv_flat.reshape(seq, heads, 2 * HEAD_DIM), cum_flat.T

    in_specs = (
        P("ep", None),
        P("ep"),
        P("ep", None, TENSOR, None),
        P("ep", TENSOR, None),
        P(),
        P(None, TENSOR),
        P(None, TENSOR),
        P(None, TENSOR),
        P(None, TENSOR),
        P(TENSOR),
        P(TENSOR, None),
        P(),
        P(None, TENSOR),
        P(None, TENSOR),
        P(TENSOR, None),
        P("ep", None, TENSOR),
        P("ep", None, TENSOR),
        P("ep", TENSOR, None),
        P("ep", None),
        P("ep", None),
    )
    out_specs = (P("ep", TENSOR), P("ep", TENSOR, None), P("ep", TENSOR))
    return jax.shard_map(shards, mesh=fine, in_specs=in_specs, out_specs=out_specs, check_vma=False)
```

```python
import jax
import jax.numpy as jnp
from jax import lax
from jax.experimental import pallas as pl
from jax.experimental.pallas import tpu as pltpu
from jax.sharding import Mesh, PartitionSpec as P

HEAD_DIM = 64
CORES = 2
LANES = 128
EPSILON = 1e-06
HUGE = 1 << 30
SHARES = (0, 4, 8, 12)
EARLY = 6
AFTER = 4
LATER = 8
TENSOR = ("ty", "tc")

f32 = jnp.float32
bf16 = jnp.bfloat16

NT = (((1,), (1,)), ((), ()))


def field(count):
    return -(-count // 8) * 8


def full_spec():
    return pl.BlockSpec(memory_space=pltpu.VMEM)


def hbm_spec():
    return pl.BlockSpec(memory_space=pltpu.HBM)


def smem_spec():
    return pl.BlockSpec(memory_space=pltpu.SMEM)


def attention_kernel(
    tokens_in,
    norm_in,
    w_forget_in,
    cum_in,
    lengths_in,
    b_forget_in,
    ids_in,
    route_in,
    w_query,
    w_key,
    w_value,
    w_output,
    cache,
    *refs,
    carried,
):
    carry_in, refs = refs[:carried], refs[carried:]
    mine_out, other_out, kv_out, cum_out, meta_out = refs[:5]
    carry_out, refs = refs[5 : 5 + carried], refs[5 + carried :]
    (
        kv_stage,
        cum_stage,
        tokens,
        norm_attn,
        w_forget,
        cum,
        lengths,
        b_forget,
        ids,
        route,
        wq_buf,
        wk_buf,
        wv_buf,
        wo_buf,
        cache_buf,
        q_rows,
        kv_rows,
        att_rows,
        bias_buf,
        shift_buf,
        score_buf,
        meta_rows,
        sem_w,
        sem_c,
        sem_n,
        sem_o,
    ) = refs
    seq, width = tokens.shape
    heads, length = cum.shape[1:]
    half_rows = cache.shape[1] // 2
    half_len = length // 2
    tiles = half_len // LANES
    span = LANES * heads
    pair = 2 * heads
    parts, _, part = mine_out.shape

    moves = (
        (tokens_in, tokens),
        (norm_in, norm_attn),
        (w_forget_in, w_forget),
        (lengths_in, lengths),
        (b_forget_in, b_forget),
        (ids_in, ids),
        (route_in, route),
        (cum_in, cum),
        (w_query, wq_buf),
        (w_key, wk_buf),
        (w_value, wv_buf),
        (w_output, wo_buf),
    )
    w_copies = [
        pltpu.make_async_copy(src, dst, sem_w.at[i]) for i, (src, dst) in enumerate(moves)
    ]
    c_copies = [
        pltpu.make_async_copy(cache.at[s], cache_buf.at[s], sem_c.at[s]) for s in range(seq)
    ]
    n_copies = [
        pltpu.make_async_copy(src, dst, sem_n.at[i])
        for i, (src, dst) in enumerate(zip(carry_in, carry_out))
    ]
    o_copies = [
        pltpu.make_async_copy(kv_stage, kv_out, sem_o.at[0]),
        pltpu.make_async_copy(cum_stage, cum_out, sem_o.at[1]),
    ]
    first = seq * SHARES[1] // 16
    queue = [*c_copies[:first], *w_copies[9:11], *c_copies[first:], w_copies[11], *n_copies]

    def launch(count):
        for copy in queue[:count]:
            copy.start()
        del queue[:count]

    for copy in w_copies[:9]:
        copy.start()
    launch(EARLY)

    sub = lax.broadcasted_iota(jnp.int32, (LANES, span), 0) * heads
    lane = lax.broadcasted_iota(jnp.int32, (LANES, span), 1)
    spread = ((lane >= sub) & (lane < sub + heads)).astype(f32).astype(bf16)
    row_id = lax.broadcasted_iota(jnp.int32, (pair, half_rows), 0)
    col_id = lax.broadcasted_iota(jnp.int32, (pair, half_rows), 1)
    place = jnp.where(
        lax.rem(row_id, heads) == lax.rem(col_id, heads),
        col_id + jnp.where(row_id >= heads, half_rows, 0),
        HUGE,
    )
    seq_lane = lax.broadcasted_iota(jnp.int32, (heads, seq), 1)
    pos_lane = lax.broadcasted_iota(jnp.int32, (heads, length), 1)
    head_row = lax.broadcasted_iota(jnp.int32, (heads, 1), 0)

    for copy in w_copies[:7]:
        copy.wait()
    launch(AFTER)
    wide = tokens[...].astype(f32)
    scale = lax.rsqrt(jnp.mean(wide * wide, axis=1, keepdims=True) + EPSILON)
    normed = (wide * scale * norm_attn[...]).astype(bf16)
    gate = lax.dot_general(w_forget[...], normed, NT, preferred_element_type=f32)
    for h in range(heads):
        gate = gate + jnp.where(head_row == h, b_forget[h], 0.0)
    forget_log = jnp.minimum(gate, 0.0) - jnp.log1p(jnp.exp(-jnp.abs(gate)))

    top_count = ids.shape[0]
    stride = field(top_count)
    meta_rows[...] = jnp.zeros_like(meta_rows)
    high = route[...].astype(bf16).astype(f32)
    middle = (route[...] - high).astype(bf16).astype(f32)
    for i, value in enumerate((ids[...].astype(f32), high, middle, route[...] - high - middle)):
        meta_rows[i * stride : i * stride + top_count, :] = value
    same = lax.broadcasted_iota(jnp.int32, (seq, seq), 0) == lax.broadcasted_iota(
        jnp.int32, (seq, seq), 1
    )
    meta_out[...] = lax.dot_general(
        same.astype(f32).astype(bf16),
        meta_rows[...].astype(bf16),
        NT,
        preferred_element_type=f32,
    ).astype(bf16)

    w_copies[7].wait()
    pieces = []
    for s in range(seq):
        rows = cum[s]
        for j in range(tiles):
            pieces.append(rows[:, j * LANES : (j + 1) * LANES])
            pieces.append(rows[:, half_len + j * LANES : half_len + (j + 1) * LANES])
    stacked = jnp.concatenate(pieces, axis=0)
    hi = stacked.astype(bf16)
    rest = stacked - hi.astype(f32)
    mid = rest.astype(bf16)
    low = (rest - mid.astype(f32)).astype(bf16)
    bias_buf[...] = (
        jnp.dot(hi, spread, preferred_element_type=f32)
        + jnp.dot(mid, spread, preferred_element_type=f32)
        + jnp.dot(low, spread, preferred_element_type=f32)
    )
    cum_all = jnp.zeros((heads, seq), f32)
    for s in range(seq):
        limit = lengths[s]
        last = jnp.sum(jnp.where(pos_lane == limit - 1, cum[s], 0.0), axis=1, keepdims=True)
        cum_new = last + forget_log[:, s : s + 1]
        cum_all = jnp.where(seq_lane == s, cum_new, cum_all)
        cum_two = jnp.concatenate([cum_new, cum_new], axis=0)
        base = s * tiles * pair
        bias = jnp.concatenate(
            [bias_buf[base + j * pair : base + (j + 1) * pair, :] for j in range(tiles)], axis=1
        )
        shift_buf[s] = jnp.where(place < limit * heads, cum_two - bias, -jnp.inf)
    cum_stage[...] = cum_all
    o_copies[1].start()

    w_copies[8].wait()
    launch(LATER)
    query = jnp.dot(normed, wq_buf[...], preferred_element_type=f32).astype(bf16).astype(f32)
    for h in range(heads):
        q_rows[pl.ds(h, seq, stride=heads), :] = jnp.concatenate(
            [
                query[:, h * HEAD_DIM : (h + 1) * HEAD_DIM] * HEAD_DIM ** (-0.5),
                jnp.zeros((seq, HEAD_DIM), f32),
            ],
            axis=1,
        )

    def project():
        w_copies[9].wait()
        w_copies[10].wait()
        key = jnp.dot(normed, wk_buf[...], preferred_element_type=f32).astype(bf16).astype(f32)
        value = jnp.dot(normed, wv_buf[...], preferred_element_type=f32).astype(bf16).astype(f32)
        for h in range(heads):
            cut = slice(h * HEAD_DIM, (h + 1) * HEAD_DIM)
            kv_rows[pl.ds(h, seq, stride=heads), :] = jnp.concatenate(
                [key[:, cut], value[:, cut]], axis=1
            )
        kv_stage[...] = kv_rows[...].astype(bf16)
        o_copies[0].start()

    def rows_of(s):
        return jnp.concatenate([cache_buf[s, :half_rows, :], cache_buf[s, half_rows:, :]], axis=1)

    def score(s):
        q_s = q_rows[s * heads : (s + 1) * heads, :]
        blank = jnp.zeros_like(q_s)
        lhs = jnp.concatenate(
            [jnp.concatenate([q_s, blank], axis=1), jnp.concatenate([blank, q_s], axis=1)], axis=0
        ).astype(bf16)
        score_buf[s] = lax.dot_general(lhs, rows_of(s), NT, preferred_element_type=f32)

    def attend(s):
        here = slice(s * heads, (s + 1) * heads)
        kv_s = kv_rows[here, :]
        own = jnp.sum(q_rows[here, :] * kv_s, axis=1, keepdims=True)
        scores = score_buf[s] + shift_buf[s]
        top = jnp.max(scores, axis=1, keepdims=True)
        top = jnp.maximum(jnp.maximum(top[:heads], top[heads:]), own)
        weights = jnp.exp(scores - jnp.concatenate([top, top], axis=0))
        weight_own = jnp.exp(own - top)
        total = jnp.sum(weights, axis=1, keepdims=True)
        inverse = 1.0 / (total[:heads] + total[heads:] + weight_own)
        probs = (weights * jnp.concatenate([inverse, inverse], axis=0)).astype(bf16)
        prob_own = (weight_own * inverse).astype(bf16).astype(f32)
        mixed = jnp.dot(probs, rows_of(s), preferred_element_type=f32)
        att_rows[here, :] = mixed[:heads, :LANES] + mixed[heads:, LANES:] + prob_own * kv_s

    bounds = [seq * share // 16 for share in SHARES]
    before = 0
    for start, stop in zip(bounds, bounds[1:] + [seq]):
        for s in range(start, stop):
            c_copies[s].wait()
        launch(len(queue))
        for s in range(start, stop):
            score(s)
        if start == 0:
            project()
        for s in range(before, start):
            attend(s)
        before = start
    for s in range(before, seq):
        attend(s)

    attended = jnp.concatenate(
        [att_rows[pl.ds(h, seq, stride=heads), :][:, HEAD_DIM:] for h in range(heads)], axis=1
    ).astype(bf16)
    w_copies[11].wait()
    core = lax.rem(lax.axis_index(TENSOR), CORES)
    for y in range(parts):
        here = pl.ds(pl.multiple_of((y * CORES + core) * part, part), part)
        mine_out[y] = jnp.dot(attended, wo_buf[:, here], preferred_element_type=f32).astype(bf16)
        there = pl.ds(pl.multiple_of((y * CORES + 1 - core) * part, part), part)
        other_out[y] = jnp.dot(attended, wo_buf[:, there], preferred_element_type=f32).astype(bf16)
    for copy in n_copies + o_copies:
        copy.wait()


def residual_kernel(*refs, groups):
    mine = refs[0]
    arrived = refs[1 : 1 + groups - 1]
    tokens, meta, packed_out, residual_out = refs[groups:]
    parts, _, part = mine.shape
    place = lax.axis_index(TENSOR)
    core = lax.rem(place, CORES)
    for y in range(parts):
        here = pl.ds(pl.multiple_of((y * CORES + core) * part, part), part)
        total = mine[y].astype(f32)
        for ref in arrived:
            total = total + ref[y].astype(f32)
        rounded = (tokens[:, here].astype(f32) + total).astype(bf16)
        for e in range(packed_out.shape[0]):
            packed_out[e, :, y * part : (y + 1) * part] = rounded

        @pl.when(place == y * CORES + core)
        def _():
            residual_out[...] = rounded

    for e in range(packed_out.shape[0]):
        packed_out[e, :, parts * part :] = meta[...]


def half_products(rows, norm_ffn, gates, ups, side, part):
    parts = rows.shape[1] // part
    squares, totals = 0.0, [0.0] * len(gates)
    for y in range(parts):
        here = pl.ds(pl.multiple_of((y * CORES + side) * part, part), part)
        piece = rows[:, y * part : (y + 1) * part].astype(f32)
        squares = squares + jnp.sum(piece * piece, axis=1, keepdims=True)
        gained = (piece * norm_ffn[:, here]).astype(bf16)
        for e, (gate, up) in enumerate(zip(gates, ups)):
            w_gate, w_up = gate[here, :], up[here, :]
            if w_gate.shape[1] % LANES == 0:
                both = jnp.dot(
                    gained, jnp.concatenate([w_gate, w_up], axis=1), preferred_element_type=f32
                )
            else:
                both = jnp.concatenate(
                    [
                        jnp.dot(gained, w_gate, preferred_element_type=f32),
                        jnp.dot(gained, w_up, preferred_element_type=f32),
                    ],
                    axis=1,
                )
            totals[e] = totals[e] + both
    return squares, totals


def near_kernel(
    near,
    norm_ffn,
    shared_gate,
    shared_up,
    expert_gate,
    expert_up,
    product_out,
    square_out,
    factor_out,
    *,
    top_count,
    seq,
    part,
):
    row_count = near.shape[0]
    experts = expert_gate.shape[0]
    half = near.shape[1] - LANES
    core = lax.rem(lax.axis_index(TENSOR), CORES)
    group = lax.axis_index("ep")
    squares, totals = half_products(
        near.at[:, :half],
        norm_ffn,
        [expert_gate.at[e] for e in range(experts)] + [shared_gate],
        [expert_up.at[e] for e in range(experts)] + [shared_up],
        core,
        part,
    )
    square_out[...] = squares
    for e, total in enumerate(totals):
        product_out[e] = total
    meta = near[:, half:].astype(f32)
    ids = meta[:, :top_count]
    stride = field(top_count)
    coef = (
        meta[:, stride : stride + top_count]
        + meta[:, 2 * stride : 2 * stride + top_count]
        + meta[:, 3 * stride : 3 * stride + top_count]
    )
    for e in range(experts):
        wanted = (group * experts + e).astype(f32)
        factor_out[e] = jnp.sum(jnp.where(ids == wanted, coef, 0.0), axis=1, keepdims=True)
    row_id = lax.broadcasted_iota(jnp.int32, (row_count, 1), 0)
    own = (row_id >= group * seq) & (row_id < (group + 1) * seq)
    factor_out[experts] = own.astype(f32)


def down_products(units, blocks):
    hidden = units[0].shape[1]
    if hidden % LANES == 0:
        return jnp.dot(
            jnp.concatenate(units, axis=1),
            jnp.concatenate(blocks, axis=0),
            preferred_element_type=f32,
        )
    total = jnp.dot(units[0], blocks[0], preferred_element_type=f32)
    for unit, block in zip(units[1:], blocks[1:]):
        total = total + jnp.dot(unit, block, preferred_element_type=f32)
    return total


def down_half(units, shared_down, expert_down, out, side):
    groups, parts, seq, part = out.shape
    for y in range(parts):
        here = pl.ds(pl.multiple_of((y * CORES + side) * part, part), part)
        blocks = [expert_down[e, :, here] for e in range(expert_down.shape[0])]
        result = down_products(units, blocks + [shared_down[:, here]])
        for g in range(groups):
            out[g, y] = result[g * seq : (g + 1) * seq].astype(out.dtype)


def far_kernel(
    far,
    products,
    near_squares,
    factors,
    norm_ffn,
    shared_gate,
    shared_up,
    shared_down,
    expert_gate,
    expert_up,
    expert_down,
    send_out,
    unit_out,
    *,
    part,
):
    experts = expert_gate.shape[0]
    hidden = expert_gate.shape[2]
    half = far.shape[1] - LANES
    side = 1 - lax.rem(lax.axis_index(TENSOR), CORES)
    squares, totals = half_products(
        far.at[:, :half],
        norm_ffn,
        [expert_gate.at[e] for e in range(experts)] + [shared_gate],
        [expert_up.at[e] for e in range(experts)] + [shared_up],
        side,
        part,
    )
    width = expert_down.shape[2]
    scale = lax.rsqrt((squares + near_squares[...]) * (1.0 / width) + EPSILON)
    units = []
    for e, total in enumerate(totals):
        both = (total + products[e]) * scale
        gate, up = both[:, :hidden], both[:, hidden:]
        units.append((gate / (1.0 + jnp.exp(-gate)) * up * factors[e]).astype(bf16))
        unit_out[e] = units[e]
    down_half(units, shared_down, expert_down, send_out, side)


def keep_kernel(units, shared_down, expert_down, keep_out):
    core = lax.rem(lax.axis_index(TENSOR), CORES)
    down_half([units[e] for e in range(units.shape[0])], shared_down, expert_down, keep_out, core)


def solution(mesh):
    groups = mesh.shape["ep"]
    tensor = mesh.shape["tp"]
    parts = tensor // CORES
    fine = Mesh(mesh.devices.reshape(groups, parts, CORES), ("ep", "ty", "tc"))

    def shards(
        tokens,
        lengths,
        cache_kv,
        cache_cum,
        norm_attn,
        w_query,
        w_key,
        w_value,
        w_forget,
        b_forget,
        w_output,
        norm_ffn,
        shared_gate,
        shared_up,
        shared_down,
        expert_gate,
        expert_up,
        expert_down,
        route_ids,
        route_weight,
    ):
        seq, width = tokens.shape
        heads, length = cache_cum.shape[1:]
        part = width // tensor
        rows = length * heads
        column = heads * HEAD_DIM
        half_shape = jax.ShapeDtypeStruct((parts, seq, part), bf16)
        carry = (shared_gate, shared_up, shared_down, expert_gate, expert_up, expert_down)
        mine, other, kv_flat, cum_flat, meta, *carry = pl.pallas_call(
            lambda *refs: attention_kernel(*refs, carried=len(carry)),
            out_shape=(
                half_shape,
                half_shape,
                jax.ShapeDtypeStruct((seq * heads, 2 * HEAD_DIM), bf16),
                jax.ShapeDtypeStruct((heads, seq), f32),
                jax.ShapeDtypeStruct((seq, LANES), bf16),
                *(jax.ShapeDtypeStruct(array.shape, array.dtype) for array in carry),
            ),
            in_specs=[hbm_spec()] * (13 + len(carry)),
            out_specs=(
                *[full_spec()] * 2,
                *[hbm_spec()] * 2,
                *[full_spec()] * (1 + len(carry)),
            ),
            scratch_shapes=[
                pltpu.VMEM((seq * heads, 2 * HEAD_DIM), bf16),
                pltpu.VMEM((heads, seq), f32),
                pltpu.VMEM((seq, width), bf16),
                pltpu.VMEM((1, width), f32),
                pltpu.VMEM((heads, width), bf16),
                pltpu.VMEM((seq, heads, length), f32),
                pltpu.SMEM((seq,), jnp.int32),
                pltpu.SMEM((heads if heads > 1 else 8,), f32),
                pltpu.VMEM(route_ids.shape[::-1], jnp.int32),
                pltpu.VMEM(route_ids.shape[::-1], f32),
                pltpu.VMEM((width, column), bf16),
                pltpu.VMEM((width, column), bf16),
                pltpu.VMEM((width, column), bf16),
                pltpu.VMEM((column, width), bf16),
                pltpu.VMEM((seq, rows, 2 * HEAD_DIM), bf16),
                pltpu.VMEM((seq * heads, 2 * HEAD_DIM), f32),
                pltpu.VMEM((seq * heads, 2 * HEAD_DIM), f32),
                pltpu.VMEM((seq * heads, 2 * HEAD_DIM), f32),
                pltpu.VMEM((seq * length // LANES * heads, LANES * heads), f32),
                pltpu.VMEM((seq, 2 * heads, rows // 2), f32),
                pltpu.VMEM((seq, 2 * heads, rows // 2), f32),
                pltpu.VMEM((LANES, seq), f32),
                pltpu.SemaphoreType.DMA((12,)),
                pltpu.SemaphoreType.DMA((seq,)),
                pltpu.SemaphoreType.DMA((len(carry),)),
                pltpu.SemaphoreType.DMA((2,)),
            ],
            compiler_params=pltpu.CompilerParams(
                vmem_limit_bytes=28 << 20
            ),
            name="attention",
        )(
            *(
                pltpu.with_memory_space_constraint(array, pltpu.HBM)
                for array in (
                    tokens,
                    norm_attn.reshape(1, width),
                    w_forget.T,
                    cache_cum,
                    lengths,
                    b_forget if heads > 1 else jnp.pad(b_forget, (0, 7)),
                    route_ids.T,
                    route_weight.T,
                    w_query,
                    w_key,
                    w_value,
                    w_output,
                    cache_kv.reshape(seq, rows, 2 * HEAD_DIM),
                    *carry,
                )
            ),
        )
        arrived = [
            lax.ppermute(
                other if k % CORES else mine, TENSOR, [(i, i ^ k) for i in range(tensor)]
            )
            for k in range(1, tensor)
        ]
        half = parts * part + LANES
        packed, residual = pl.pallas_call(
            lambda *refs: residual_kernel(*refs, groups=tensor),
            out_shape=(
                jax.ShapeDtypeStruct((groups, seq, half), bf16),
                jax.ShapeDtypeStruct((seq, part), bf16),
            ),
            in_specs=[full_spec()] * (tensor + 2),
            out_specs=(full_spec(),) * 2,
            compiler_params=pltpu.CompilerParams(vmem_limit_bytes=4 << 20),
            name="residual",
        )(mine, *arrived, tokens, meta)
        near = lax.all_to_all(packed, "ep", split_axis=0, concat_axis=0, tiled=True)
        near = near.reshape(groups * seq, half)
        far = lax.ppermute(near, TENSOR, [(i, i ^ 1) for i in range(tensor)])
        experts, _, hidden = expert_gate.shape
        row_count = groups * seq
        gain = norm_ffn.reshape(1, width)
        s_gate, s_up, s_down, e_gate, e_up, e_down = carry
        small = pltpu.CompilerParams(vmem_limit_bytes=8 << 20)
        products, squares, factors = pl.pallas_call(
            lambda *refs: near_kernel(
                *refs, top_count=route_ids.shape[1], seq=seq, part=part
            ),
            out_shape=(
                jax.ShapeDtypeStruct((experts + 1, row_count, 2 * hidden), f32),
                jax.ShapeDtypeStruct((row_count, 1), f32),
                jax.ShapeDtypeStruct((experts + 1, row_count, 1), f32),
            ),
            in_specs=[full_spec()] * 6,
            out_specs=(full_spec(),) * 3,
            compiler_params=small,
            name="near",
        )(near, gain, s_gate, s_up, e_gate, e_up)
        send, units = pl.pallas_call(
            lambda *refs: far_kernel(*refs, part=part),
            out_shape=(
                jax.ShapeDtypeStruct((groups, parts, seq, part), bf16),
                jax.ShapeDtypeStruct((experts + 1, row_count, hidden), bf16),
            ),
            in_specs=[full_spec()] * 11,
            out_specs=(full_spec(),) * 2,
            compiler_params=small,
            name="far",
        )(far, products, squares, factors, gain, *carry)
        swapped = lax.ppermute(send, TENSOR, [(i, i ^ 1) for i in range(tensor)])
        keep = pl.pallas_call(
            keep_kernel,
            out_shape=jax.ShapeDtypeStruct((groups, parts, seq, part), f32),
            in_specs=[full_spec()] * 3,
            out_specs=full_spec(),
            compiler_params=small,
            name="keep",
        )(units, s_down, e_down)
        chip = (keep + swapped.astype(f32)).astype(bf16)
        pieces = lax.all_to_all(
            chip.reshape(groups * parts, seq, part),
            ("ep", "ty"),
            split_axis=0,
            concat_axis=0,
            tiled=True,
        )
        output = (residual.astype(f32) + jnp.sum(pieces.astype(f32), axis=0)).astype(bf16)
        return output, kv_flat.reshape(seq, heads, 2 * HEAD_DIM), cum_flat.T

    in_specs = (
        P("ep", None),
        P("ep"),
        P("ep", None, TENSOR, None),
        P("ep", TENSOR, None),
        P(),
        P(None, TENSOR),
        P(None, TENSOR),
        P(None, TENSOR),
        P(None, TENSOR),
        P(TENSOR),
        P(TENSOR, None),
        P(),
        P(None, TENSOR),
        P(None, TENSOR),
        P(TENSOR, None),
        P("ep", None, TENSOR),
        P("ep", None, TENSOR),
        P("ep", TENSOR, None),
        P("ep", None),
        P("ep", None),
    )
    out_specs = (P("ep", TENSOR), P("ep", TENSOR, None), P("ep", TENSOR))
    return jax.shard_map(shards, mesh=fine, in_specs=in_specs, out_specs=out_specs, check_vma=False)
```

```python
import jax
import jax.numpy as jnp
from jax import lax
from jax.experimental import pallas as pl
from jax.experimental.pallas import tpu as pltpu
from jax.sharding import Mesh, PartitionSpec as P

HEAD_DIM = 64
CORES = 2
LANES = 128
EPSILON = 1e-06
HUGE = 1 << 30
SHARES = (0, 4, 8, 12)
EARLY = 6
AFTER = 2
LATER = 10
TENSOR = ("ty", "tc")

f32 = jnp.float32
bf16 = jnp.bfloat16

NT = (((1,), (1,)), ((), ()))


def field(count):
    return -(-count // 8) * 8


def full_spec():
    return pl.BlockSpec(memory_space=pltpu.VMEM)


def hbm_spec():
    return pl.BlockSpec(memory_space=pltpu.HBM)


def smem_spec():
    return pl.BlockSpec(memory_space=pltpu.SMEM)


def attention_kernel(
    tokens_in,
    norm_in,
    w_forget_in,
    cum_in,
    lengths_in,
    b_forget_in,
    ids_in,
    route_in,
    w_query,
    w_key,
    w_value,
    w_output,
    cache,
    *refs,
    carried,
):
    carry_in, refs = refs[:carried], refs[carried:]
    mine_out, other_out, kv_out, cum_out, meta_out = refs[:5]
    carry_out, refs = refs[5 : 5 + carried], refs[5 + carried :]
    (
        kv_stage,
        cum_stage,
        tokens,
        norm_attn,
        w_forget,
        cum,
        lengths,
        b_forget,
        ids,
        route,
        wq_buf,
        wk_buf,
        wv_buf,
        wo_buf,
        cache_buf,
        q_rows,
        kv_rows,
        att_rows,
        bias_buf,
        shift_buf,
        score_buf,
        meta_rows,
        sem_w,
        sem_c,
        sem_n,
        sem_o,
    ) = refs
    seq, width = tokens.shape
    heads, length = cum.shape[1:]
    half_rows = cache.shape[1] // 2
    half_len = length // 2
    tiles = half_len // LANES
    span = LANES * heads
    pair = 2 * heads
    parts, _, part = mine_out.shape

    moves = (
        (tokens_in, tokens),
        (norm_in, norm_attn),
        (w_forget_in, w_forget),
        (lengths_in, lengths),
        (b_forget_in, b_forget),
        (ids_in, ids),
        (route_in, route),
        (cum_in, cum),
        (w_query, wq_buf),
        (w_key, wk_buf),
        (w_value, wv_buf),
        (w_output, wo_buf),
    )
    w_copies = [
        pltpu.make_async_copy(src, dst, sem_w.at[i]) for i, (src, dst) in enumerate(moves)
    ]
    c_copies = [
        pltpu.make_async_copy(cache.at[s], cache_buf.at[s], sem_c.at[s]) for s in range(seq)
    ]
    n_copies = [
        pltpu.make_async_copy(src, dst, sem_n.at[i])
        for i, (src, dst) in enumerate(zip(carry_in, carry_out))
    ]
    o_copies = [
        pltpu.make_async_copy(kv_stage, kv_out, sem_o.at[0]),
        pltpu.make_async_copy(cum_stage, cum_out, sem_o.at[1]),
    ]
    first = seq * SHARES[1] // 16
    queue = [*c_copies[:first], *w_copies[9:11], *c_copies[first:], w_copies[11], *n_copies]

    def launch(count):
        for copy in queue[:count]:
            copy.start()
        del queue[:count]

    for copy in w_copies[:9]:
        copy.start()
    launch(EARLY)

    sub = lax.broadcasted_iota(jnp.int32, (LANES, span), 0) * heads
    lane = lax.broadcasted_iota(jnp.int32, (LANES, span), 1)
    spread = ((lane >= sub) & (lane < sub + heads)).astype(f32).astype(bf16)
    row_id = lax.broadcasted_iota(jnp.int32, (pair, half_rows), 0)
    col_id = lax.broadcasted_iota(jnp.int32, (pair, half_rows), 1)
    place = jnp.where(
        lax.rem(row_id, heads) == lax.rem(col_id, heads),
        col_id + jnp.where(row_id >= heads, half_rows, 0),
        HUGE,
    )
    seq_lane = lax.broadcasted_iota(jnp.int32, (heads, seq), 1)
    pos_lane = lax.broadcasted_iota(jnp.int32, (heads, length), 1)
    head_row = lax.broadcasted_iota(jnp.int32, (heads, 1), 0)

    for copy in w_copies[:7]:
        copy.wait()
    launch(AFTER)
    wide = tokens[...].astype(f32)
    scale = lax.rsqrt(jnp.mean(wide * wide, axis=1, keepdims=True) + EPSILON)
    normed = (wide * scale * norm_attn[...]).astype(bf16)
    gate = lax.dot_general(w_forget[...], normed, NT, preferred_element_type=f32)
    for h in range(heads):
        gate = gate + jnp.where(head_row == h, b_forget[h], 0.0)
    forget_log = jnp.minimum(gate, 0.0) - jnp.log1p(jnp.exp(-jnp.abs(gate)))

    top_count = ids.shape[0]
    stride = field(top_count)
    meta_rows[...] = jnp.zeros_like(meta_rows)
    high = route[...].astype(bf16).astype(f32)
    middle = (route[...] - high).astype(bf16).astype(f32)
    for i, value in enumerate((ids[...].astype(f32), high, middle, route[...] - high - middle)):
        meta_rows[i * stride : i * stride + top_count, :] = value
    same = lax.broadcasted_iota(jnp.int32, (seq, seq), 0) == lax.broadcasted_iota(
        jnp.int32, (seq, seq), 1
    )
    meta_out[...] = lax.dot_general(
        same.astype(f32).astype(bf16),
        meta_rows[...].astype(bf16),
        NT,
        preferred_element_type=f32,
    ).astype(bf16)

    w_copies[7].wait()
    pieces = []
    for s in range(seq):
        rows = cum[s]
        for j in range(tiles):
            pieces.append(rows[:, j * LANES : (j + 1) * LANES])
            pieces.append(rows[:, half_len + j * LANES : half_len + (j + 1) * LANES])
    stacked = jnp.concatenate(pieces, axis=0)
    hi = stacked.astype(bf16)
    rest = stacked - hi.astype(f32)
    mid = rest.astype(bf16)
    low = (rest - mid.astype(f32)).astype(bf16)
    bias_buf[...] = (
        jnp.dot(hi, spread, preferred_element_type=f32)
        + jnp.dot(mid, spread, preferred_element_type=f32)
        + jnp.dot(low, spread, preferred_element_type=f32)
    )
    cum_all = jnp.zeros((heads, seq), f32)
    for s in range(seq):
        limit = lengths[s]
        last = jnp.sum(jnp.where(pos_lane == limit - 1, cum[s], 0.0), axis=1, keepdims=True)
        cum_new = last + forget_log[:, s : s + 1]
        cum_all = jnp.where(seq_lane == s, cum_new, cum_all)
        cum_two = jnp.concatenate([cum_new, cum_new], axis=0)
        base = s * tiles * pair
        bias = jnp.concatenate(
            [bias_buf[base + j * pair : base + (j + 1) * pair, :] for j in range(tiles)], axis=1
        )
        shift_buf[s] = jnp.where(place < limit * heads, cum_two - bias, -jnp.inf)
    cum_stage[...] = cum_all
    o_copies[1].start()

    w_copies[8].wait()
    launch(LATER)
    query = jnp.dot(normed, wq_buf[...], preferred_element_type=f32).astype(bf16).astype(f32)
    for h in range(heads):
        q_rows[pl.ds(h, seq, stride=heads), :] = jnp.concatenate(
            [
                query[:, h * HEAD_DIM : (h + 1) * HEAD_DIM] * HEAD_DIM ** (-0.5),
                jnp.zeros((seq, HEAD_DIM), f32),
            ],
            axis=1,
        )

    def project():
        w_copies[9].wait()
        w_copies[10].wait()
        key = jnp.dot(normed, wk_buf[...], preferred_element_type=f32).astype(bf16).astype(f32)
        value = jnp.dot(normed, wv_buf[...], preferred_element_type=f32).astype(bf16).astype(f32)
        for h in range(heads):
            cut = slice(h * HEAD_DIM, (h + 1) * HEAD_DIM)
            kv_rows[pl.ds(h, seq, stride=heads), :] = jnp.concatenate(
                [key[:, cut], value[:, cut]], axis=1
            )
        kv_stage[...] = kv_rows[...].astype(bf16)
        o_copies[0].start()

    def rows_of(s):
        return jnp.concatenate([cache_buf[s, :half_rows, :], cache_buf[s, half_rows:, :]], axis=1)

    def score(s):
        q_s = q_rows[s * heads : (s + 1) * heads, :]
        blank = jnp.zeros_like(q_s)
        lhs = jnp.concatenate(
            [jnp.concatenate([q_s, blank], axis=1), jnp.concatenate([blank, q_s], axis=1)], axis=0
        ).astype(bf16)
        score_buf[s] = lax.dot_general(lhs, rows_of(s), NT, preferred_element_type=f32)

    def attend(s):
        here = slice(s * heads, (s + 1) * heads)
        kv_s = kv_rows[here, :]
        own = jnp.sum(q_rows[here, :] * kv_s, axis=1, keepdims=True)
        scores = score_buf[s] + shift_buf[s]
        top = jnp.max(scores, axis=1, keepdims=True)
        top = jnp.maximum(jnp.maximum(top[:heads], top[heads:]), own)
        weights = jnp.exp(scores - jnp.concatenate([top, top], axis=0))
        weight_own = jnp.exp(own - top)
        total = jnp.sum(weights, axis=1, keepdims=True)
        inverse = 1.0 / (total[:heads] + total[heads:] + weight_own)
        probs = (weights * jnp.concatenate([inverse, inverse], axis=0)).astype(bf16)
        prob_own = (weight_own * inverse).astype(bf16).astype(f32)
        mixed = jnp.dot(probs, rows_of(s), preferred_element_type=f32)
        att_rows[here, :] = mixed[:heads, :LANES] + mixed[heads:, LANES:] + prob_own * kv_s

    bounds = [seq * share // 16 for share in SHARES]
    before = 0
    for start, stop in zip(bounds, bounds[1:] + [seq]):
        for s in range(start, stop):
            c_copies[s].wait()
        launch(len(queue))
        for s in range(start, stop):
            score(s)
        if start == 0:
            project()
        for s in range(before, start):
            attend(s)
        before = start
    for s in range(before, seq):
        attend(s)

    attended = jnp.concatenate(
        [att_rows[pl.ds(h, seq, stride=heads), :][:, HEAD_DIM:] for h in range(heads)], axis=1
    ).astype(bf16)
    w_copies[11].wait()
    core = lax.rem(lax.axis_index(TENSOR), CORES)
    for y in range(parts):
        here = pl.ds(pl.multiple_of((y * CORES + core) * part, part), part)
        mine_out[y] = jnp.dot(attended, wo_buf[:, here], preferred_element_type=f32).astype(bf16)
        there = pl.ds(pl.multiple_of((y * CORES + 1 - core) * part, part), part)
        other_out[y] = jnp.dot(attended, wo_buf[:, there], preferred_element_type=f32).astype(bf16)
    for copy in n_copies + o_copies:
        copy.wait()


def residual_kernel(*refs, groups):
    mine = refs[0]
    arrived = refs[1 : 1 + groups - 1]
    tokens, meta, packed_out, residual_out = refs[groups:]
    parts, _, part = mine.shape
    place = lax.axis_index(TENSOR)
    core = lax.rem(place, CORES)
    for y in range(parts):
        here = pl.ds(pl.multiple_of((y * CORES + core) * part, part), part)
        total = mine[y].astype(f32)
        for ref in arrived:
            total = total + ref[y].astype(f32)
        rounded = (tokens[:, here].astype(f32) + total).astype(bf16)
        for e in range(packed_out.shape[0]):
            packed_out[e, :, y * part : (y + 1) * part] = rounded

        @pl.when(place == y * CORES + core)
        def _():
            residual_out[...] = rounded

    for e in range(packed_out.shape[0]):
        packed_out[e, :, parts * part :] = meta[...]


def half_products(rows, norm_ffn, gates, ups, side, part):
    parts = rows.shape[1] // part
    squares, totals = 0.0, [0.0] * len(gates)
    for y in range(parts):
        here = pl.ds(pl.multiple_of((y * CORES + side) * part, part), part)
        piece = rows[:, y * part : (y + 1) * part].astype(f32)
        squares = squares + jnp.sum(piece * piece, axis=1, keepdims=True)
        gained = (piece * norm_ffn[:, here]).astype(bf16)
        for e, (gate, up) in enumerate(zip(gates, ups)):
            w_gate, w_up = gate[here, :], up[here, :]
            if w_gate.shape[1] % LANES == 0:
                both = jnp.dot(
                    gained, jnp.concatenate([w_gate, w_up], axis=1), preferred_element_type=f32
                )
            else:
                both = jnp.concatenate(
                    [
                        jnp.dot(gained, w_gate, preferred_element_type=f32),
                        jnp.dot(gained, w_up, preferred_element_type=f32),
                    ],
                    axis=1,
                )
            totals[e] = totals[e] + both
    return squares, totals


def near_kernel(
    near,
    norm_ffn,
    shared_gate,
    shared_up,
    expert_gate,
    expert_up,
    product_out,
    square_out,
    factor_out,
    *,
    top_count,
    seq,
    part,
):
    row_count = near.shape[0]
    experts = expert_gate.shape[0]
    half = near.shape[1] - LANES
    core = lax.rem(lax.axis_index(TENSOR), CORES)
    group = lax.axis_index("ep")
    squares, totals = half_products(
        near.at[:, :half],
        norm_ffn,
        [expert_gate.at[e] for e in range(experts)] + [shared_gate],
        [expert_up.at[e] for e in range(experts)] + [shared_up],
        core,
        part,
    )
    square_out[...] = squares
    for e, total in enumerate(totals):
        product_out[e] = total
    meta = near[:, half:].astype(f32)
    ids = meta[:, :top_count]
    stride = field(top_count)
    coef = (
        meta[:, stride : stride + top_count]
        + meta[:, 2 * stride : 2 * stride + top_count]
        + meta[:, 3 * stride : 3 * stride + top_count]
    )
    for e in range(experts):
        wanted = (group * experts + e).astype(f32)
        factor_out[e] = jnp.sum(jnp.where(ids == wanted, coef, 0.0), axis=1, keepdims=True)
    row_id = lax.broadcasted_iota(jnp.int32, (row_count, 1), 0)
    own = (row_id >= group * seq) & (row_id < (group + 1) * seq)
    factor_out[experts] = own.astype(f32)


def down_products(units, blocks):
    hidden = units[0].shape[1]
    if hidden % LANES == 0:
        return jnp.dot(
            jnp.concatenate(units, axis=1),
            jnp.concatenate(blocks, axis=0),
            preferred_element_type=f32,
        )
    total = jnp.dot(units[0], blocks[0], preferred_element_type=f32)
    for unit, block in zip(units[1:], blocks[1:]):
        total = total + jnp.dot(unit, block, preferred_element_type=f32)
    return total


def down_half(units, shared_down, expert_down, out, side):
    groups, parts, seq, part = out.shape
    for y in range(parts):
        here = pl.ds(pl.multiple_of((y * CORES + side) * part, part), part)
        blocks = [expert_down[e, :, here] for e in range(expert_down.shape[0])]
        result = down_products(units, blocks + [shared_down[:, here]])
        for g in range(groups):
            out[g, y] = result[g * seq : (g + 1) * seq].astype(out.dtype)


def far_kernel(
    far,
    products,
    near_squares,
    factors,
    norm_ffn,
    shared_gate,
    shared_up,
    shared_down,
    expert_gate,
    expert_up,
    expert_down,
    send_out,
    unit_out,
    *,
    part,
):
    experts = expert_gate.shape[0]
    hidden = expert_gate.shape[2]
    half = far.shape[1] - LANES
    side = 1 - lax.rem(lax.axis_index(TENSOR), CORES)
    squares, totals = half_products(
        far.at[:, :half],
        norm_ffn,
        [expert_gate.at[e] for e in range(experts)] + [shared_gate],
        [expert_up.at[e] for e in range(experts)] + [shared_up],
        side,
        part,
    )
    width = expert_down.shape[2]
    scale = lax.rsqrt((squares + near_squares[...]) * (1.0 / width) + EPSILON)
    units = []
    for e, total in enumerate(totals):
        both = (total + products[e]) * scale
        gate, up = both[:, :hidden], both[:, hidden:]
        units.append((gate / (1.0 + jnp.exp(-gate)) * up * factors[e]).astype(bf16))
        unit_out[e] = units[e]
    down_half(units, shared_down, expert_down, send_out, side)


def keep_kernel(units, shared_down, expert_down, keep_out):
    core = lax.rem(lax.axis_index(TENSOR), CORES)
    down_half([units[e] for e in range(units.shape[0])], shared_down, expert_down, keep_out, core)


def solution(mesh):
    groups = mesh.shape["ep"]
    tensor = mesh.shape["tp"]
    parts = tensor // CORES
    fine = Mesh(mesh.devices.reshape(groups, parts, CORES), ("ep", "ty", "tc"))

    def shards(
        tokens,
        lengths,
        cache_kv,
        cache_cum,
        norm_attn,
        w_query,
        w_key,
        w_value,
        w_forget,
        b_forget,
        w_output,
        norm_ffn,
        shared_gate,
        shared_up,
        shared_down,
        expert_gate,
        expert_up,
        expert_down,
        route_ids,
        route_weight,
    ):
        seq, width = tokens.shape
        heads, length = cache_cum.shape[1:]
        part = width // tensor
        rows = length * heads
        column = heads * HEAD_DIM
        half_shape = jax.ShapeDtypeStruct((parts, seq, part), bf16)
        carry = (shared_gate, shared_up, shared_down, expert_gate, expert_up, expert_down)
        mine, other, kv_flat, cum_flat, meta, *carry = pl.pallas_call(
            lambda *refs: attention_kernel(*refs, carried=len(carry)),
            out_shape=(
                half_shape,
                half_shape,
                jax.ShapeDtypeStruct((seq * heads, 2 * HEAD_DIM), bf16),
                jax.ShapeDtypeStruct((heads, seq), f32),
                jax.ShapeDtypeStruct((seq, LANES), bf16),
                *(jax.ShapeDtypeStruct(array.shape, array.dtype) for array in carry),
            ),
            in_specs=[hbm_spec()] * (13 + len(carry)),
            out_specs=(
                *[full_spec()] * 2,
                *[hbm_spec()] * 2,
                *[full_spec()] * (1 + len(carry)),
            ),
            scratch_shapes=[
                pltpu.VMEM((seq * heads, 2 * HEAD_DIM), bf16),
                pltpu.VMEM((heads, seq), f32),
                pltpu.VMEM((seq, width), bf16),
                pltpu.VMEM((1, width), f32),
                pltpu.VMEM((heads, width), bf16),
                pltpu.VMEM((seq, heads, length), f32),
                pltpu.SMEM((seq,), jnp.int32),
                pltpu.SMEM((heads if heads > 1 else 8,), f32),
                pltpu.VMEM(route_ids.shape[::-1], jnp.int32),
                pltpu.VMEM(route_ids.shape[::-1], f32),
                pltpu.VMEM((width, column), bf16),
                pltpu.VMEM((width, column), bf16),
                pltpu.VMEM((width, column), bf16),
                pltpu.VMEM((column, width), bf16),
                pltpu.VMEM((seq, rows, 2 * HEAD_DIM), bf16),
                pltpu.VMEM((seq * heads, 2 * HEAD_DIM), f32),
                pltpu.VMEM((seq * heads, 2 * HEAD_DIM), f32),
                pltpu.VMEM((seq * heads, 2 * HEAD_DIM), f32),
                pltpu.VMEM((seq * length // LANES * heads, LANES * heads), f32),
                pltpu.VMEM((seq, 2 * heads, rows // 2), f32),
                pltpu.VMEM((seq, 2 * heads, rows // 2), f32),
                pltpu.VMEM((LANES, seq), f32),
                pltpu.SemaphoreType.DMA((12,)),
                pltpu.SemaphoreType.DMA((seq,)),
                pltpu.SemaphoreType.DMA((len(carry),)),
                pltpu.SemaphoreType.DMA((2,)),
            ],
            compiler_params=pltpu.CompilerParams(
                vmem_limit_bytes=28 << 20
            ),
            name="attention",
        )(
            *(
                pltpu.with_memory_space_constraint(array, pltpu.HBM)
                for array in (
                    tokens,
                    norm_attn.reshape(1, width),
                    w_forget.T,
                    cache_cum,
                    lengths,
                    b_forget if heads > 1 else jnp.pad(b_forget, (0, 7)),
                    route_ids.T,
                    route_weight.T,
                    w_query,
                    w_key,
                    w_value,
                    w_output,
                    cache_kv.reshape(seq, rows, 2 * HEAD_DIM),
                    *carry,
                )
            ),
        )
        arrived = [
            lax.ppermute(
                other if k % CORES else mine, TENSOR, [(i, i ^ k) for i in range(tensor)]
            )
            for k in range(1, tensor)
        ]
        half = parts * part + LANES
        packed, residual = pl.pallas_call(
            lambda *refs: residual_kernel(*refs, groups=tensor),
            out_shape=(
                jax.ShapeDtypeStruct((groups, seq, half), bf16),
                jax.ShapeDtypeStruct((seq, part), bf16),
            ),
            in_specs=[full_spec()] * (tensor + 2),
            out_specs=(full_spec(),) * 2,
            compiler_params=pltpu.CompilerParams(vmem_limit_bytes=4 << 20),
            name="residual",
        )(mine, *arrived, tokens, meta)
        near = lax.all_to_all(packed, "ep", split_axis=0, concat_axis=0, tiled=True)
        near = near.reshape(groups * seq, half)
        far = lax.ppermute(near, TENSOR, [(i, i ^ 1) for i in range(tensor)])
        experts, _, hidden = expert_gate.shape
        row_count = groups * seq
        gain = norm_ffn.reshape(1, width)
        s_gate, s_up, s_down, e_gate, e_up, e_down = carry
        small = pltpu.CompilerParams(
            vmem_limit_bytes=8 << 20
        )
        products, squares, factors = pl.pallas_call(
            lambda *refs: near_kernel(
                *refs, top_count=route_ids.shape[1], seq=seq, part=part
            ),
            out_shape=(
                jax.ShapeDtypeStruct((experts + 1, row_count, 2 * hidden), f32),
                jax.ShapeDtypeStruct((row_count, 1), f32),
                jax.ShapeDtypeStruct((experts + 1, row_count, 1), f32),
            ),
            in_specs=[full_spec()] * 6,
            out_specs=(full_spec(),) * 3,
            compiler_params=small,
            name="near",
        )(near, gain, s_gate, s_up, e_gate, e_up)
        send, units = pl.pallas_call(
            lambda *refs: far_kernel(*refs, part=part),
            out_shape=(
                jax.ShapeDtypeStruct((groups, parts, seq, part), bf16),
                jax.ShapeDtypeStruct((experts + 1, row_count, hidden), bf16),
            ),
            in_specs=[full_spec()] * 11,
            out_specs=(full_spec(),) * 2,
            compiler_params=small,
            name="far",
        )(far, products, squares, factors, gain, *carry)
        swapped = lax.ppermute(send, TENSOR, [(i, i ^ 1) for i in range(tensor)])
        keep = pl.pallas_call(
            keep_kernel,
            out_shape=jax.ShapeDtypeStruct((groups, parts, seq, part), f32),
            in_specs=[full_spec()] * 3,
            out_specs=full_spec(),
            compiler_params=small,
            name="keep",
        )(units, s_down, e_down)
        chip = (keep + swapped.astype(f32)).astype(bf16)
        pieces = lax.all_to_all(
            chip.reshape(groups * parts, seq, part),
            ("ep", "ty"),
            split_axis=0,
            concat_axis=0,
            tiled=True,
        )
        output = (residual.astype(f32) + jnp.sum(pieces.astype(f32), axis=0)).astype(bf16)
        return output, kv_flat.reshape(seq, heads, 2 * HEAD_DIM), cum_flat.T

    in_specs = (
        P("ep", None),
        P("ep"),
        P("ep", None, TENSOR, None),
        P("ep", TENSOR, None),
        P(),
        P(None, TENSOR),
        P(None, TENSOR),
        P(None, TENSOR),
        P(None, TENSOR),
        P(TENSOR),
        P(TENSOR, None),
        P(),
        P(None, TENSOR),
        P(None, TENSOR),
        P(TENSOR, None),
        P("ep", None, TENSOR),
        P("ep", None, TENSOR),
        P("ep", TENSOR, None),
        P("ep", None),
        P("ep", None),
    )
    out_specs = (P("ep", TENSOR), P("ep", TENSOR, None), P("ep", TENSOR))
    return jax.shard_map(shards, mesh=fine, in_specs=in_specs, out_specs=out_specs, check_vma=False)
```
